256 devices in a mesh: ep: 64 (over z, y, core), tp: 4 (over x).
Axes of the slice: x: 4, y: 4, z: 8, core: 2. Of those that a mesh axis runs over, the one named last changes fastest.
Arguments:
- mixer_channels_raw: bfloat16 [24576, 4096], P('ep', 'tp'), may hold values from -6 to 6
- write_vectors_raw: bfloat16 [24576, 2048], P('ep', 'tp'), may hold values from -6 to 6
- read_vectors_raw: bfloat16 [24576, 2048], P('ep', 'tp'), may hold values from -6 to 6
- gate_logits: bfloat16 [24576, 4096], P('ep', 'tp'), may hold values from -6 to 6
- step_size_raw: bfloat16 [24576, 64], P('ep', 'tp'), may hold values from -4 to 4
- extra_log_decay: float32 [24576, 64], P('ep', 'tp'), may hold values from -2 to 0, as said below
- mixer_conv_taps: float32 [4, 4096], P(None, 'tp'), may hold values from -3 to 3
- write_conv_taps: float32 [4, 2048], P(None, 'tp'), may hold values from -3 to 3
- read_conv_taps: float32 [4, 2048], P(None, 'tp'), may hold values from -3 to 3
- step_size_bias: float32 [64], P('tp'), may hold values from -5 to -3
- log_decay_rate: float32 [64], P('tp'), as said below
- direct_path_weight: float32 [64], P('tp'), may hold values from 0.5 to 3
- mixer_output_weight: bfloat16 [4096, 2048], P('tp'), may hold values from -0.09375 to 0.09375
- mixer_norm_scale: float32 [2048], replicated, may hold values from 0.1 to 1.9
- routed_tokens: bfloat16 [16384, 2048], P('ep'), may hold values from -6 to 6
- expert_norm_scale: float32 [2048], replicated, may hold values from 0.1 to 1.9
- routes: int32 [16384, 2], P('ep'), may hold values from 0 to 63, as said below
- routing_weights: float32 [16384, 2], P('ep'), may hold values from 0.2 to 1
- expert_gate_matrix: bfloat16 [64, 2048, 1024], P('ep', None, 'tp'), may hold values from -0.125 to 0.125
- expert_up_matrix: bfloat16 [64, 2048, 1024], P('ep', None, 'tp'), may hold values from -0.125 to 0.125
- expert_down_matrix: bfloat16 [64, 1024, 2048], P('ep', 'tp'), may hold values from -0.1875 to 0.1875
Outputs:
- mixer_out: bfloat16 [24576, 2048], P(('ep', 'tp'))
- expert_out: bfloat16 [16384, 2048], P('ep', 'tp')
The draws below stay inside these ranges and needn't reach their ends.
Inputs may be any that keep to these rules, and one draw needn't show every extreme that they name: `routes`: each row names two different experts of one group of 4 consecutive experts. In each aligned block of 256 rows no expert is named by more than 16 rows, and some expert is named by exactly 16 rows in every block. `extra_log_decay`: zero at all but a few positions. `log_decay_rate`: logarithms of positive rates.
All inputs are finite; a program needn't handle non-finite values.
Results may differ from the reference program's by a relative error of at most 0.019.
Values may be sent and summed in bfloat16 or wider, within the bound.
No kernel may reach another device: no remote copies, remote signals or barrier semaphores. Data moves between devices by JAX's collectives and lax.ppermute only.
A program may use at most 128 MiB of HBM per device.

```python
import jax
import jax.numpy as jnp
from jax import lax

D = 2048
HEADS = 64
HEAD_DIM = 64
DI = 4096
GROUPS = 16
STATE = 128
CONV = 4
BLOCK = 128
TOKA_DEV = 384
SEQ_A = 24576
FF = 1024
EPG = 4
EXPERTS = 64
TOKB_DEV = 256
TOKENS_B = 16384
CAP = 16
N_EP = 64
N_TP = 4


def draw_step_size_raw(key, part):
    subkeys = jax.random.split(key, 2)
    blocks = SEQ_A // TOKA_DEV
    offset = jax.random.uniform(subkeys[0], (blocks, 1, HEADS), jnp.float32, -0.7, 0.7)
    noise = jnp.clip(0.6 * jax.random.normal(subkeys[1], (blocks, TOKA_DEV, HEADS), jnp.float32), -3.0, 3.0)
    return (noise + offset).reshape(SEQ_A, HEADS).astype(jnp.bfloat16)


def draw_log_decay_rate(key, part):
    subkeys = jax.random.split(key, 3)
    chance = 0.5
    fast_heads = jax.random.uniform(subkeys[0], (HEADS,), jnp.float32) < chance
    slow_rate = jax.random.uniform(subkeys[1], (HEADS,), jnp.float32, 0.2, 0.6) / (SEQ_A * 0.03)
    fast_rate = jax.random.uniform(subkeys[2], (HEADS,), jnp.float32, 1.0, 4.0)
    return jnp.log(jnp.where(fast_heads, fast_rate, slow_rate))


def draw_extra_log_decay(key, part):
    subkeys = jax.random.split(key, 2)
    places = jax.random.randint(subkeys[0], (3,), 0, SEQ_A)
    depths = jax.random.uniform(subkeys[1], (3, HEADS), jnp.float32, -0.69, -0.22)
    return jnp.zeros((SEQ_A, HEADS), jnp.float32).at[places].add(depths)


def draw_routes(key, part):
    nblocks = TOKENS_B // TOKB_DEV
    ngroups = EXPERTS // EPG
    span = TOKB_DEV // ngroups
    label_key = jax.random.fold_in(key, 7)
    labels = jax.vmap(lambda group: jax.random.permutation(jax.random.fold_in(label_key, group), EPG))(jnp.arange(ngroups, dtype=jnp.int32))

    def one_block(number):
        ranks = jax.random.permutation(jax.random.fold_in(key, number), TOKB_DEV).astype(jnp.int32)
        group = ranks // span
        within = ranks % span
        first = labels[group, 0]
        second = labels[group, 1 + within % (EPG - 1)]
        return jnp.stack([group * EPG + first, group * EPG + second], axis=1)
    return jax.vmap(one_block)(jnp.arange(nblocks, dtype=jnp.int32)).reshape(TOKENS_B, 2).astype(jnp.int32)


def levels(key, dims, cuts, smallest, top_value):
    loudness = 1.0
    for position, shards_of in cuts:
        draws = jax.random.uniform(jax.random.fold_in(jax.random.fold_in(key, 6), position), (shards_of,), jnp.float32, smallest / len(cuts), top_value / len(cuts))
        loudness = loudness * jnp.repeat(jnp.exp(draws), dims[position] // shards_of).reshape((-1,) + (1,) * (len(dims) - 1 - position))
    return loudness


def gaussian(stream_key, extent, scale, reach, shards=(), kind=jnp.bfloat16):
    level = levels(stream_key, extent, shards, -0.22, 0.18) if shards else 1.0
    values = jax.random.normal(stream_key, extent, jnp.float32) * scale * level
    return jnp.minimum(jnp.maximum(values, -reach), reach).astype(kind)


def setup_inputs(seed: int = 0) -> dict:
    keys = jax.random.split(jax.random.key(seed), 22)
    return {
        "mixer_channels_raw": gaussian(keys[0], (SEQ_A, DI), 1.0, 6.0, ((0, 64), (1, 4))),
        "write_vectors_raw": gaussian(keys[1], (SEQ_A, GROUPS * STATE), 1.0, 6.0, ((0, 64), (1, 4))),
        "read_vectors_raw": gaussian(keys[2], (SEQ_A, GROUPS * STATE), 1.0, 6.0, ((0, 64), (1, 4))),
        "gate_logits": gaussian(keys[3], (SEQ_A, DI), 1.0, 6.0, ((0, 64), (1, 4))),
        "step_size_raw": draw_step_size_raw(jax.random.fold_in(keys[21], 71), 0),
        "extra_log_decay": draw_extra_log_decay(jax.random.fold_in(keys[21], 71), 0),
        "mixer_conv_taps": gaussian(keys[6], (CONV, DI), 0.5, 3.0, ((1, 4),), jnp.float32),
        "write_conv_taps": gaussian(keys[7], (CONV, GROUPS * STATE), 0.5, 3.0, ((1, 4),), jnp.float32),
        "read_conv_taps": gaussian(keys[8], (CONV, GROUPS * STATE), 0.5, 3.0, ((1, 4),), jnp.float32),
        "step_size_bias": jnp.clip(-5.0 + 2.0 * jax.random.uniform(keys[9], (HEADS,), jnp.float32) ** levels(keys[9], (HEADS,), ((0, 4),), -0.2, 0.2), -5.0, -3.0),
        "log_decay_rate": draw_log_decay_rate(jax.random.fold_in(keys[21], 71), 0),
        "direct_path_weight": jnp.clip(0.5 + 2.5 * jax.random.uniform(keys[11], (HEADS,), jnp.float32) ** levels(keys[11], (HEADS,), ((0, 4),), -0.2, 0.2), 0.5, 3.0),
        "mixer_output_weight": gaussian(keys[12], (DI, D), DI ** -0.5, 0.09375, ((0, 4),)),
        "mixer_norm_scale": jnp.clip(1.0 + 0.18 * jax.random.normal(keys[13], (D,), jnp.float32), 0.1, 1.9),
        "routed_tokens": gaussian(keys[14], (TOKENS_B, D), 1.0, 6.0, ((0, 64),)),
        "expert_norm_scale": jnp.clip(1.0 + 0.18 * jax.random.normal(keys[15], (D,), jnp.float32), 0.1, 1.9),
        "routes": draw_routes(jax.random.fold_in(keys[21], 71), 0),
        "routing_weights": jnp.clip(0.2 + 0.8 * jax.random.uniform(keys[17], (TOKENS_B, 2), jnp.float32) ** levels(keys[17], (TOKENS_B, 2), ((0, 64),), -0.2, 0.2), 0.2, 1.0),
        "expert_gate_matrix": gaussian(keys[18], (EXPERTS, D, FF), D ** -0.5, 0.125, ((0, 64), (2, 4))),
        "expert_up_matrix": gaussian(keys[19], (EXPERTS, D, FF), D ** -0.5, 0.125, ((0, 64), (2, 4))),
        "expert_down_matrix": gaussian(keys[20], (EXPERTS, FF, D), FF ** -0.5, 0.1875, ((0, 64), (1, 4))),
    }


eps = 1e-06
highest = lax.Precision.HIGHEST

def causal_conv(values, taps):
    margin = taps.shape[0] - 1
    length = values.shape[0]
    joined = jnp.concatenate([jnp.zeros((margin, values.shape[1]), jnp.float32), values.astype(jnp.float32)], axis=0)
    summed = jnp.zeros((length, values.shape[1]), jnp.float32)
    for offset in range(taps.shape[0]):
        summed = summed + taps[offset][None, :] * joined[offset:offset + length]
    return jax.nn.silu(summed)

def normalize(values, gain):
    return values * lax.rsqrt(lax.optimization_barrier(jnp.mean(values * values, axis=-1, keepdims=True)) + eps) * gain[None, :]

def block_terms(state, inputs):
    inner, step_size, decay_factor, write, read = inputs
    length = inner.shape[0]
    groups = write.shape[1]
    inner = inner.reshape(length, groups, -1, inner.shape[2])
    step_size = step_size.reshape(length, groups, -1)
    cumul = jnp.cumsum(decay_factor, axis=0).reshape(length, groups, -1)
    causal = jnp.arange(length)[:, None] >= jnp.arange(length)[None, :]
    spread = jnp.where(causal[:, :, None, None], cumul[:, None] - cumul[None, :], -jnp.inf)
    weights = jnp.exp(spread) * step_size[None]
    intersection = jnp.einsum('lgn,sgn->lsg', read, write, precision=highest)
    within = jnp.einsum('lsgr,sgrp->lgrp', intersection[..., None] * weights, inner, precision=highest)
    carried = jnp.einsum('lgn,grpn->lgrp', read, state, precision=highest) * jnp.exp(cumul)[..., None]
    tail = jnp.exp(cumul[-1][None] - cumul) * step_size
    update = jnp.einsum('sgn,sgrp->grpn', write, inner * tail[..., None], precision=highest)
    state = jnp.exp(cumul[-1])[..., None, None] * state + update
    return (state, (within + carried).reshape(length, -1))

def reference(mixer_channels_raw, write_vectors_raw, read_vectors_raw, gate_logits, step_size_raw, extra_log_decay, mixer_conv_taps, write_conv_taps, read_conv_taps, step_size_bias, log_decay_rate, direct_path_weight, mixer_output_weight, mixer_norm_scale, routed_tokens, expert_norm_scale, routes, routing_weights, expert_gate_matrix, expert_up_matrix, expert_down_matrix):
    inner = causal_conv(mixer_channels_raw, mixer_conv_taps)
    write = causal_conv(write_vectors_raw, write_conv_taps)
    read = causal_conv(read_vectors_raw, read_conv_taps)
    step_size = jax.nn.softplus(step_size_raw.astype(jnp.float32) + step_size_bias[None, :])
    decay_factor = extra_log_decay - step_size * jnp.exp(log_decay_rate)[None, :]
    nblocks = SEQ_A // BLOCK
    ratio = HEADS // GROUPS
    start_state = jnp.zeros((GROUPS, ratio, HEAD_DIM, STATE), jnp.float32)
    inputs = (inner.reshape(nblocks, BLOCK, HEADS, HEAD_DIM), step_size.reshape(nblocks, BLOCK, HEADS), decay_factor.reshape(nblocks, BLOCK, HEADS), write.reshape(nblocks, BLOCK, GROUPS, STATE), read.reshape(nblocks, BLOCK, GROUPS, STATE))
    final_state, outputs = lax.scan(block_terms, start_state, inputs)
    scanned = outputs.reshape(SEQ_A, DI) + inner * jnp.repeat(direct_path_weight, HEAD_DIM)[None, :]
    gated = (scanned * jax.nn.silu(gate_logits.astype(jnp.float32))).astype(jnp.bfloat16)
    share = DI // N_TP
    projected = jnp.zeros((SEQ_A, D), jnp.float32)
    for shard in range(N_TP):
        piece = jnp.dot(gated[:, shard * share:(shard + 1) * share], mixer_output_weight[shard * share:(shard + 1) * share], preferred_element_type=jnp.float32).astype(jnp.bfloat16)
        projected = projected + lax.optimization_barrier(piece).astype(jnp.float32)
    mixer_out = normalize(projected, mixer_norm_scale).astype(jnp.bfloat16)
    moe_normed = normalize(routed_tokens.astype(jnp.float32), expert_norm_scale).astype(jnp.bfloat16)
    flat_expert = routes.reshape(-1).astype(jnp.int32)
    onehot = (flat_expert[:, None] == jnp.arange(EXPERTS, dtype=jnp.int32)[None, :]).astype(jnp.int32)
    rank = lax.optimization_barrier(jnp.sum(jnp.cumsum(onehot, axis=0) * onehot, axis=1)) - 1
    slots_total = N_EP * CAP
    dest = (flat_expert * slots_total + rank).astype(jnp.int32)
    token_ids = jnp.repeat(jnp.arange(TOKENS_B, dtype=jnp.int32), 2)
    slot_token = jnp.full((EXPERTS * slots_total,), TOKENS_B, jnp.int32).at[dest].set(token_ids)
    slot_weight = jnp.zeros((EXPERTS * slots_total,), jnp.float32).at[dest].set(routing_weights.reshape(-1))
    padded_rows = jnp.concatenate([moe_normed, jnp.zeros((1, D), jnp.bfloat16)], axis=0)
    hidden_share = FF // N_TP

    def expert_pass(summed, inputs):
        gate_w, up_w, down_w, tokens_here, weight_here = inputs
        chosen = padded_rows[tokens_here]
        gate_val = jnp.dot(chosen, gate_w, preferred_element_type=jnp.float32)
        up_val = jnp.dot(chosen, up_w, preferred_element_type=jnp.float32)
        hidden = (jax.nn.silu(gate_val) * up_val).astype(jnp.bfloat16)
        result = jnp.zeros((chosen.shape[0], D), jnp.float32)
        for shard in range(N_TP):
            piece = jnp.dot(hidden[:, shard * hidden_share:(shard + 1) * hidden_share], down_w[shard * hidden_share:(shard + 1) * hidden_share], preferred_element_type=jnp.float32).astype(jnp.bfloat16)
            result = result + lax.optimization_barrier(piece).astype(jnp.float32)
        rounded = lax.optimization_barrier(result.astype(jnp.bfloat16)).astype(jnp.float32)
        return (summed.at[tokens_here].add(rounded * weight_here[:, None]), None)
    summed, unused = lax.scan(expert_pass, jnp.zeros((TOKENS_B + 1, D), jnp.float32), (expert_gate_matrix, expert_up_matrix, expert_down_matrix, slot_token.reshape(EXPERTS, slots_total), slot_weight.reshape(EXPERTS, slots_total)))
    expert_out = summed[:TOKENS_B].astype(jnp.bfloat16)
    return (mixer_out, expert_out)
```

```python
import jax
import jax.numpy as jnp
from jax import lax
from jax.experimental import pallas as pl
from jax.experimental.pallas import tpu as pltpu
from jax.sharding import Mesh
from jax.sharding import PartitionSpec as P


HEAD_DIM = 64
STATE = 128
CAP = 16
EP = ("ep_0", "ep_1", "ep_2")
PLANE = ("ep_1", "ep_2")
EP_TP = ("ep_0", "ep_1", "ep_2", "tp")
EPS = 1e-06
HI = lax.Precision.HIGHEST
F32 = jnp.float32
BF16 = jnp.bfloat16
MIB = 1024 * 1024


def vmem(count):
    return [pl.BlockSpec(memory_space=pltpu.VMEM)] * count


def params(mib):
    return pltpu.CompilerParams(vmem_limit_bytes=mib * MIB)


def cost(flops, nbytes):
    return pl.CostEstimate(flops=flops, bytes_accessed=nbytes, transcendentals=0)


def iota(shape, dim):
    return lax.broadcasted_iota(jnp.int32, shape, dim)


def spread_heads(group, heads, width):
    per = width // HEAD_DIM
    return (iota((heads, width), 0) == group * per + iota((heads, width), 1) // HEAD_DIM).astype(F32)


def dot(a, b, precision=None):
    return jnp.dot(a, b, preferred_element_type=F32, precision=precision)


def dot_tn(a, b):
    return lax.dot_general(a, b, (((0,), (0,)), ((), ())), preferred_element_type=F32)


def dot_nt(a, b):
    return lax.dot_general(a, b, (((1,), (1,)), ((), ())), preferred_element_type=F32)


def silu(x):
    return x / (1.0 + jnp.exp(-x))


def conv_kernel(
    ch_ref, wr_ref, rd_ref, edge_ref, ct_ref, wt_ref, rt_ref, sraw_ref, extra_ref, bias_ref, rate_ref,
    x_ref, w_ref, r_ref, pay_ref, cum_ref, step_ref,
):
    length, heads = sraw_ref.shape
    tile = 128

    def conv(src, taps, dst, first):
        def body(i, carry):
            lanes = pl.ds(pl.multiple_of(i * tile, tile), tile)
            edges = edge_ref[:, pl.ds(pl.multiple_of(first + i * tile, tile), tile)].astype(F32)
            joined = jnp.concatenate([edges[8:16], src[:, lanes].astype(F32)], axis=0)
            t = taps[:, lanes]
            total = t[0:1] * joined[5 : 5 + length]
            for k in range(1, t.shape[0]):
                total = total + t[k : k + 1] * joined[5 + k : 5 + k + length]
            dst[:, lanes] = silu(total).astype(BF16)
            return carry

        lax.fori_loop(0, src.shape[1] // tile, body, 0)

    nch, nw = ch_ref.shape[1], wr_ref.shape[1]
    conv(ch_ref, ct_ref, x_ref, 0)
    conv(wr_ref, wt_ref, w_ref, nch)
    conv(rd_ref, rt_ref, r_ref, nch + nw)

    raw = sraw_ref[...].astype(F32) + bias_ref[...]
    step = jnp.maximum(raw, 0.0) + jnp.log1p(jnp.exp(-jnp.abs(raw)))
    decay = extra_ref[...] - step * jnp.exp(rate_ref[...])
    below = (iota((length, length), 0) >= iota((length, length), 1)).astype(F32)
    cum = dot(below, decay, HI)
    cum_ref[...] = cum
    step_ref[...] = step
    last = cum[length - 1 : length]
    tail = jnp.exp(last - cum) * step
    groups = nw // STATE
    width = nch // groups
    parts = pay_ref.shape[0]
    rows = STATE // parts
    his, los = [], []
    for g in range(groups):
        spread = spread_heads(g, heads, width)
        xt = (x_ref[:, g * width : (g + 1) * width].astype(F32) * dot(tail, spread, HI)).astype(BF16)
        state = dot_tn(w_ref[:, g * STATE : (g + 1) * STATE], xt).astype(BF16)
        pay_ref[:, g * rows : (g + 1) * rows, :] = state.reshape(parts, rows, width)
        total = dot(last, spread, HI)
        high = total.astype(BF16).astype(F32)
        his.append(high)
        los.append(total - high)
    extra_rows = jnp.concatenate(his + los + [jnp.zeros((16 - 2 * groups, width), F32)], axis=0).astype(BF16)
    for p in range(parts):
        pay_ref[p, groups * rows :, :] = extra_rows


def within_kernel(x_ref, w_ref, r_ref, cum_ref, step_ref, direct_ref, y_ref):
    g = pl.program_id(0)
    length, heads = cum_ref.shape
    width = x_ref.shape[1]
    per = width // HEAD_DIM
    block = 128
    pick = (iota((heads, 128), 0) == g * per + iota((heads, 128), 1)).astype(F32)
    cols = dot(cum_ref[...], pick, HI)
    rows = cols.T
    x = x_ref[...].astype(F32)
    xs = (x * dot(step_ref[...], spread_heads(g, heads, width), HI)).astype(BF16)
    first_half = iota((block, 128), 1) < HEAD_DIM
    for i in range(length // block):
        here = slice(i * block, (i + 1) * block)
        seen = (i + 1) * block
        gram = dot_nt(r_ref[here, :], w_ref[0:seen, :])
        causal = i * block + iota((block, seen), 0) >= iota((block, seen), 1)
        outs = []
        for j in range(per):
            gap = cols[here, j : j + 1] - rows[j : j + 1, 0:seen]
            m = (gram * jnp.exp(jnp.where(causal, gap, -1e30))).astype(BF16)
            pair = (j // 2) * 128
            outs.append(dot(m, xs[0:seen, pair : pair + 128]))
        for q in range(per // 2):
            lanes = slice(q * 128, (q + 1) * 128)
            y_ref[here, lanes] = (
                jnp.where(first_half, outs[2 * q], outs[2 * q + 1]) + direct_ref[:, lanes] * x[here, lanes]
            )


def plane_kernel(z_ref, before_ref, total_ref):
    parts, height, width = z_ref.shape
    groups = 4
    rows = (height - 16) // groups
    base = groups * rows
    his, los = [], []
    for g in range(groups):
        run = jnp.zeros((rows, width), F32)
        log = jnp.zeros((1, width), F32)
        here = slice(g * rows, (g + 1) * rows)
        for p in range(parts):
            before_ref[p, here, :] = run
            before_ref[p, base + g : base + g + 1, :] = log
            pad = z_ref[p, base : base + 16, :].astype(F32)
            own = pad[g : g + 1] + pad[groups + g : groups + g + 1]
            run = jnp.exp(own) * run + z_ref[p, here, :].astype(F32)
            log = log + own
        total_ref[here, :] = run.astype(BF16)
        high = log.astype(BF16).astype(F32)
        his.append(high)
        los.append(log - high)
    total_ref[base:, :] = jnp.concatenate(
        his + los + [jnp.zeros((16 - 2 * groups, width), F32)], axis=0
    ).astype(BF16)


def enter_kernel(zi_ref, before_ref, planes_ref, out_ref):
    count, height, width = planes_ref.shape
    parts = before_ref.shape[0]
    groups = 4
    rows = (height - 16) // groups
    base = groups * rows
    mine = zi_ref[0]
    for g in range(groups):
        here = slice(g * rows, (g + 1) * rows)
        state = jnp.zeros((rows, width), F32)
        for k in range(count):
            pad = planes_ref[k, base : base + 16, :].astype(F32)
            own = pad[g : g + 1] + pad[groups + g : groups + g + 1]
            new = jnp.exp(own) * state + planes_ref[k, here, :].astype(F32)
            state = jnp.where(k < mine, new, state)
        for p in range(parts):
            log = before_ref[p, base + g : base + g + 1, :]
            out_ref[p, here, :] = (before_ref[p, here, :] + jnp.exp(log) * state).astype(BF16)


def project_kernel(
    me_ref, y_ref, r_ref, s_ref, cum_ref, gate_ref, wo_ref,
    own_ref, up_ref, down_ref, opa_ref, opb_ref, gated_ref,
):
    length, heads = cum_ref.shape
    n = 4
    part = length // n
    groups = r_ref.shape[1] // STATE
    width = y_ref.shape[1] // groups

    @pl.when(pl.program_id(0) == 0)
    def _():
        me = me_ref[0]
        states = [
            s_ref[:, g * 16 : (g + 1) * 16, :].reshape(STATE, width) for g in range(groups)
        ]
        for k in range(n):
            rows = pl.ds(pl.multiple_of(lax.rem(me + k, n) * part, part), part)
            grown = jnp.exp(cum_ref[rows, :])
            for g in range(groups):
                lanes = slice(g * width, (g + 1) * width)
                carried = dot(r_ref[rows, g * STATE : (g + 1) * STATE], states[g])
                y = y_ref[rows, lanes] + dot(grown, spread_heads(g, heads, width), HI) * carried
                gate = gate_ref[rows, lanes].astype(F32)
                gated_ref[k * part : (k + 1) * part, lanes] = (y * silu(gate)).astype(BF16)

    out = dot(gated_ref[...], wo_ref[...]).astype(BF16)
    own_ref[...] = out[0:part]
    up_ref[...] = out[part : 2 * part]
    opa_ref[...] = out[2 * part : 2 * part + part // 2]
    opb_ref[...] = out[2 * part + part // 2 : 3 * part]
    down_ref[...] = out[3 * part : 4 * part]


def norm_kernel(own_ref, u_ref, d_ref, gain_ref, out_ref):
    total = own_ref[...].astype(F32) + u_ref[...].astype(F32) + d_ref[...].astype(F32)
    mean = jnp.mean(total * total, axis=-1, keepdims=True)
    out_ref[...] = (total * lax.rsqrt(mean + EPS) * gain_ref[...]).astype(BF16)


def dispatch_kernel(me_ref, tok_ref, gain_ref, routes_ref, out_ref, dest_ref, normed_ref):
    count = tok_ref.shape[0]
    slots, quarter = out_ref.shape
    experts = slots // CAP
    v = tok_ref[...].astype(F32)
    mean = jnp.mean(v * v, axis=-1, keepdims=True)
    normed_ref[...] = (v * lax.rsqrt(mean + EPS) * gain_ref[...]).astype(BF16)
    first, second = routes_ref[:, 0:1], routes_ref[:, 1:2]
    ids = iota((count, experts), 1)
    is_first, is_second = ids == first, ids == second
    named = jnp.where(is_first | is_second, 1.0, 0.0).astype(BF16)
    before = jnp.where(iota((count, count), 0) > iota((count, count), 1), 1.0, 0.0).astype(BF16)
    rank = dot(before, named)
    place = rank + (ids * CAP).astype(F32)
    dest0 = jnp.sum(jnp.where(is_first, place, 0.0), axis=1, keepdims=True).astype(jnp.int32)
    dest1 = jnp.sum(jnp.where(is_second, place, 0.0), axis=1, keepdims=True).astype(jnp.int32)
    dest_ref[:, 0:1] = dest0
    dest_ref[:, 1:2] = dest1
    slot = iota((count, slots), 1)
    chosen = jnp.where((slot == dest0) | (slot == dest1), 1.0, 0.0).astype(BF16)
    lanes = pl.ds(pl.multiple_of(me_ref[0] * quarter, quarter), quarter)
    out_ref[...] = dot_tn(chosen, normed_ref[:, lanes]).astype(BF16)


def combine_kernel(back_ref, dest_ref, weight_ref, out_ref):
    count = dest_ref.shape[0]
    slot = iota((count, back_ref.shape[0]), 1)
    mix = jnp.where(slot == dest_ref[:, 0:1], weight_ref[:, 0:1], 0.0) + jnp.where(
        slot == dest_ref[:, 1:2], weight_ref[:, 1:2], 0.0
    )
    high = mix.astype(BF16)
    low = (mix - high.astype(F32)).astype(BF16)
    back = back_ref[...]
    out_ref[...] = (dot(high, back) + dot(low, back)).astype(BF16)


def ring_dot(me, pieces, weights):
    own, left, right, op0, op1 = pieces
    size = own.shape[1]
    half = size // 2

    def rows(shift, offset, count):
        start = lax.rem(me + shift, 4) * size + offset
        return pl.ds(pl.multiple_of(start, half), count)

    out = []
    for w in weights:
        total = dot(own[...], w[rows(0, 0, size), :])
        total = total + dot(left[...], w[rows(3, 0, size), :])
        total = total + dot(right[...], w[rows(1, 0, size), :])
        total = total + dot(op0[...], w[rows(2, 0, half), :])
        total = total + dot(op1[...], w[rows(2, half, half), :])
        out.append(total)
    return out


def hidden_kernel(me_ref, own, left, right, op0, op1, gate_ref, up_ref, out_ref):
    gate, up = ring_dot(me_ref[0], (own, left, right, op0, op1), (gate_ref, up_ref))
    out_ref[...] = (silu(gate) * up).astype(BF16)


def result_kernel(me_ref, own, left, right, op0, op1, down_ref, out_ref):
    (total,) = ring_dot(me_ref[0], (own, left, right, op0, op1), (down_ref,))
    out_ref[...] = total.astype(BF16)


def ring_pieces(x, axis):
    n = lax.axis_size(axis)
    plus = [(i, (i + 1) % n) for i in range(n)]
    minus = [(i, (i - 1) % n) for i in range(n)]
    half = x.shape[1] // 2
    left = lax.ppermute(x, axis, plus)
    right = lax.ppermute(x, axis, minus)
    op0 = lax.ppermute(left[:, :half], axis, plus)
    op1 = lax.ppermute(right[:, half:], axis, minus)
    return x, left, right, op0, op1


def ring_call(kernel, me, pieces, weights, columns, tile):
    rows = pieces[0].shape[0]
    smem = pl.BlockSpec(memory_space=pltpu.SMEM)
    specs = [smem]
    specs += [pl.BlockSpec((tile, p.shape[1]), lambda i: (i, 0)) for p in pieces]
    specs += [pl.BlockSpec(w.shape, lambda i: (0, 0)) for w in weights]
    depth = weights[0].shape[0]
    return pl.pallas_call(
        kernel,
        grid=(rows // tile,),
        in_specs=specs,
        out_specs=pl.BlockSpec((tile, columns), lambda i: (i, 0)),
        out_shape=jax.ShapeDtypeStruct((rows, columns), BF16),
        compiler_params=params(32),
        cost_estimate=cost(2 * rows * depth * columns * len(weights), rows * depth * 2),
    )(me, *pieces, *weights)


def per_device(
    mixer_channels_raw,
    write_vectors_raw,
    read_vectors_raw,
    gate_logits,
    step_size_raw,
    extra_log_decay,
    mixer_conv_taps,
    write_conv_taps,
    read_conv_taps,
    step_size_bias,
    log_decay_rate,
    direct_path_weight,
    mixer_output_weight,
    mixer_norm_scale,
    routed_tokens,
    expert_norm_scale,
    routes,
    routing_weights,
    expert_gate_matrix,
    expert_up_matrix,
    expert_down_matrix,
):
    sds = jax.ShapeDtypeStruct
    smem = pl.BlockSpec(memory_space=pltpu.SMEM)
    tp = lax.axis_index("tp")
    me = tp.reshape(1).astype(jnp.int32)
    tps = lax.axis_size("tp")
    plus = [(i, (i + 1) % tps) for i in range(tps)]
    minus = [(i, (i - 1) % tps) for i in range(tps)]
    cross = [(i, (i + 2) % tps) for i in range(tps)]

    tokens, model = routed_tokens.shape
    experts = lax.axis_size(EP)
    slots = experts * CAP
    quarter = model // tps
    outgoing, dest = pl.pallas_call(
        dispatch_kernel,
        in_specs=[smem] + vmem(3),
        out_specs=vmem(2),
        out_shape=(sds((slots, quarter), BF16), sds((tokens, 2), jnp.int32)),
        scratch_shapes=[pltpu.VMEM((tokens, model), BF16)],
        compiler_params=params(24),
        cost_estimate=cost(2 * slots * tokens * quarter, 4 * MIB),
        name="dispatch",
    )(me, routed_tokens, expert_norm_scale[None, :], routes)
    arrived = lax.all_to_all(
        outgoing.reshape(experts, CAP, quarter), EP, split_axis=0, concat_axis=0, tiled=True
    )
    arrived = arrived.reshape(slots, quarter)

    ff = expert_down_matrix.shape[1]
    down = expert_down_matrix[0]

    def feature_block(shift):
        return lax.dynamic_slice(down, (0, lax.rem(tp + shift, tps) * quarter), (ff, quarter))

    d_own = feature_block(0)
    d_left = lax.ppermute(feature_block(1), "tp", plus)
    d_right = lax.ppermute(feature_block(3), "tp", minus)
    d_cross = lax.ppermute(feature_block(2), "tp", cross)

    length, channels = mixer_channels_raw.shape
    heads = step_size_raw.shape[1]
    nw = write_vectors_raw.shape[1]
    groups = nw // STATE
    width = channels // groups
    edge = jnp.concatenate(
        [mixer_channels_raw[-16:], write_vectors_raw[-16:], read_vectors_raw[-16:]], axis=1
    )
    edge = lax.ppermute(edge, EP, [(i, i + 1) for i in range(experts - 1)])
    parts = lax.axis_size(PLANE)
    height = groups * (STATE // parts) + 16
    x, w, r, payload, cum, step = pl.pallas_call(
        conv_kernel,
        in_specs=vmem(11),
        out_specs=vmem(6),
        out_shape=(
            sds((length, channels), BF16),
            sds((length, nw), BF16),
            sds((length, nw), BF16),
            sds((parts, height, width), BF16),
            sds((length, heads), F32),
            sds((length, heads), F32),
        ),
        compiler_params=params(24),
        cost_estimate=cost(2 * length * STATE * channels * 8, 4 * MIB),
        name="conv",
    )(
        mixer_channels_raw,
        write_vectors_raw,
        read_vectors_raw,
        edge,
        mixer_conv_taps,
        write_conv_taps,
        read_conv_taps,
        step_size_raw,
        extra_log_decay,
        step_size_bias[None, :],
        log_decay_rate[None, :],
    )
    gathered = lax.all_to_all(payload, PLANE, 0, 0, tiled=True)
    before, total = pl.pallas_call(
        plane_kernel,
        in_specs=vmem(1),
        out_specs=vmem(2),
        out_shape=(sds((parts, height, width), F32), sds((height, width), BF16)),
        compiler_params=params(8),
        cost_estimate=cost(1000000, MIB),
        name="plane",
    )(gathered)
    zs = lax.axis_size("ep_0")
    planes = lax.all_to_all(
        jnp.broadcast_to(total[None], (zs, height, width)), "ep_0", 0, 0, tiled=True
    )
    entering = pl.pallas_call(
        enter_kernel,
        in_specs=[smem] + vmem(2),
        out_specs=vmem(1)[0],
        out_shape=sds((parts, height - 16, width), BF16),
        compiler_params=params(8),
        cost_estimate=cost(1000000, MIB),
        name="enter",
    )(lax.axis_index("ep_0").reshape(1).astype(jnp.int32), before, planes)
    entering = lax.all_to_all(entering, PLANE, 0, 0, tiled=True)

    y = pl.pallas_call(
        within_kernel,
        grid=(groups,),
        in_specs=[
            pl.BlockSpec((length, width), lambda g: (0, g)),
            pl.BlockSpec((length, STATE), lambda g: (0, g)),
            pl.BlockSpec((length, STATE), lambda g: (0, g)),
            pl.BlockSpec((length, heads), lambda g: (0, 0)),
            pl.BlockSpec((length, heads), lambda g: (0, 0)),
            pl.BlockSpec((1, width), lambda g: (0, g)),
        ],
        out_specs=pl.BlockSpec((length, width), lambda g: (0, g)),
        out_shape=sds((length, channels), F32),
        compiler_params=params(24),
        cost_estimate=cost(4 * length * length * channels, 4 * MIB),
        name="within",
    )(x, w, r, cum, step, jnp.repeat(direct_path_weight, HEAD_DIM)[None, :])

    out_dim = mixer_output_weight.shape[1]
    part = length // tps
    tile = 512
    row_block = lambda rows: pl.BlockSpec((rows, tile), lambda j: (0, j))
    whole = lambda a: pl.BlockSpec(a.shape, lambda j: (0,) * a.ndim)
    own, up, dn, opa, opb = pl.pallas_call(
        project_kernel,
        grid=(out_dim // tile,),
        in_specs=[smem]
        + [whole(a) for a in (y, r, entering, cum, gate_logits)]
        + [pl.BlockSpec((channels, tile), lambda j: (0, j))],
        out_specs=(row_block(part), row_block(part), row_block(part), row_block(part // 2), row_block(part // 2)),
        out_shape=(
            sds((part, out_dim), BF16),
            sds((part, out_dim), BF16),
            sds((part, out_dim), BF16),
            sds((part // 2, out_dim), BF16),
            sds((part // 2, out_dim), BF16),
        ),
        scratch_shapes=[pltpu.VMEM((length, channels), BF16)],
        compiler_params=params(24),
        cost_estimate=cost(2 * length * channels * out_dim, 6 * MIB),
        name="project",
    )(me, y, r, entering, cum, gate_logits, mixer_output_weight)
    opa = lax.ppermute(opa, "tp", plus)
    opb = lax.ppermute(opb, "tp", minus)
    half = part // 2
    up = jnp.concatenate([(up[:half].astype(F32) + opa.astype(F32)).astype(BF16), up[half:]], axis=0)
    dn = jnp.concatenate([dn[:half], (dn[half:].astype(F32) + opb.astype(F32)).astype(BF16)], axis=0)
    up = lax.ppermute(up, "tp", plus)
    dn = lax.ppermute(dn, "tp", minus)
    mixer_out = pl.pallas_call(
        norm_kernel,
        in_specs=vmem(4),
        out_specs=vmem(1)[0],
        out_shape=sds((part, out_dim), BF16),
        compiler_params=params(8),
        cost_estimate=cost(1000000, 2 * MIB),
        name="norm",
    )(own, up, dn, mixer_norm_scale[None, :])

    pieces = ring_pieces(arrived, "tp")
    hidden = ring_call(
        hidden_kernel, me, pieces, (expert_gate_matrix[0], expert_up_matrix[0]), ff, 256
    )
    stacked = jnp.zeros((tps, ff, quarter), BF16)
    for shift, block in ((0, d_own), (3, d_left), (1, d_right), (2, d_cross)):
        stacked = lax.dynamic_update_slice(stacked, block[None], (lax.rem(tp + shift, tps), 0, 0))
    pieces = ring_pieces(hidden, "tp")
    result = ring_call(
        result_kernel, me, pieces, (stacked.reshape(tps * ff, quarter),), quarter, 256
    )
    returned = lax.all_to_all(
        result.reshape(experts, CAP, quarter), EP, split_axis=0, concat_axis=0, tiled=True
    )
    returned = returned.reshape(slots, quarter)
    expert_out = pl.pallas_call(
        combine_kernel,
        in_specs=vmem(3),
        out_specs=vmem(1)[0],
        out_shape=sds((tokens, quarter), BF16),
        compiler_params=params(16),
        cost_estimate=cost(4 * slots * tokens * quarter, 2 * MIB),
        name="combine",
    )(returned, dest, routing_weights)
    return (mixer_out, expert_out)


def solution(mesh):
    split = Mesh(mesh.devices.reshape(8, 4, 2, mesh.shape["tp"]), EP_TP)
    placed = (
        P(EP, "tp"),
        P(EP, "tp"),
        P(EP, "tp"),
        P(EP, "tp"),
        P(EP, "tp"),
        P(EP, "tp"),
        P(None, "tp"),
        P(None, "tp"),
        P(None, "tp"),
        P("tp"),
        P("tp"),
        P("tp"),
        P("tp", None),
        P(),
        P(EP, None),
        P(),
        P(EP, None),
        P(EP, None),
        P(EP, None, "tp"),
        P(EP, None, "tp"),
        P(EP, "tp", None),
    )

    return jax.shard_map(
        per_device,
        mesh=split,
        in_specs=placed,
        out_specs=(P(EP_TP, None), P(EP, "tp")),
        check_vma=False,
    )
```

```python
import jax
import jax.numpy as jnp
from jax import lax
from jax.experimental import pallas as pl
from jax.experimental.pallas import tpu as pltpu
from jax.sharding import Mesh
from jax.sharding import PartitionSpec as P


HEAD_DIM = 64
STATE = 128
CAP = 16
EP = ("ep_0", "ep_1", "ep_2")
PLANE = ("ep_1", "ep_2")
EP_TP = ("ep_0", "ep_1", "ep_2", "tp")
EPS = 1e-06
F32 = jnp.float32
BF16 = jnp.bfloat16
MIB = 1024 * 1024
BIG = 56
MID = 24


def vmem(count):
    return [pl.BlockSpec(memory_space=pltpu.VMEM)] * count


def params(mib):
    return pltpu.CompilerParams(vmem_limit_bytes=mib * MIB)


def cost(flops, nbytes):
    return pl.CostEstimate(flops=flops, bytes_accessed=nbytes, transcendentals=0)


def iota(shape, dim):
    return lax.broadcasted_iota(jnp.int32, shape, dim)


def spread_heads(group, heads, width):
    per = width // HEAD_DIM
    return (iota((heads, width), 0) == group * per + iota((heads, width), 1) // HEAD_DIM).astype(F32)


def dot(a, b, precision=None):
    return jnp.dot(a, b, preferred_element_type=F32, precision=precision)


def dot_tn(a, b):
    return lax.dot_general(a, b, (((0,), (0,)), ((), ())), preferred_element_type=F32)


def dot_nt(a, b):
    return lax.dot_general(a, b, (((1,), (1,)), ((), ())), preferred_element_type=F32)


def silu(x):
    return 0.5 * x * (1.0 + jnp.tanh(0.5 * x))


def split3(x):
    high = x.astype(BF16)
    rest = x - high.astype(F32)
    middle = rest.astype(BF16)
    low = (rest - middle.astype(F32)).astype(BF16)
    return jnp.concatenate([high, middle, low], axis=0)


def to_lanes(terms, mask):
    return dot_tn(terms, jnp.concatenate([mask.astype(BF16)] * 3, axis=0))


def to_column(row):
    n = row.shape[1]
    return jnp.sum(jnp.where(iota((n, n), 0) == iota((n, n), 1), row, 0.0), axis=1, keepdims=True)


def conv_kernel(
    place_ref, ch_ref, wr_ref, rd_ref, edge_ref, ct_ref, wt_ref, rt_ref, sraw_ref, extra_ref, bias_ref, rate_ref,
    x_ref, w_ref, r_ref, cum_ref, step_ref, *rest,
):
    *block_refs, pay_ref = rest
    heads, length = sraw_ref.shape
    tile = 128

    def conv(src, taps, dst, first):
        def body(i, carry):
            lanes = pl.ds(pl.multiple_of(i * tile, tile), tile)
            edges = edge_ref[:, pl.ds(pl.multiple_of(first + i * tile, tile), tile)].astype(F32)
            joined = jnp.concatenate([edges[8:16], src[:, lanes].astype(F32)], axis=0)
            t = taps[:, lanes]
            total = t[0:1] * joined[5 : 5 + length]
            for k in range(1, t.shape[0]):
                total = total + t[k : k + 1] * joined[5 + k : 5 + k + length]
            dst[:, lanes] = silu(total).astype(BF16)
            return carry

        lax.fori_loop(0, src.shape[1] // tile, body, 0)

    nch, nw = ch_ref.shape[1], wr_ref.shape[1]
    conv(ch_ref, ct_ref, x_ref, 0)
    conv(wr_ref, wt_ref, w_ref, nch)
    conv(rd_ref, rt_ref, r_ref, nch + nw)

    raw = sraw_ref[...].astype(F32) + to_column(bias_ref[...])
    step = jnp.maximum(raw, 0.0) + jnp.log1p(jnp.exp(-jnp.abs(raw)))
    decay = extra_ref[...] - step * to_column(jnp.exp(rate_ref[...]))
    upto = jnp.where(iota((length, length), 0) <= iota((length, length), 1), 1.0, 0.0).astype(BF16)
    sums = dot(split3(decay), upto)
    cum = sums[0:heads] + sums[heads : 2 * heads] + sums[2 * heads :]
    cum_ref[...] = cum
    step_ref[...] = step
    last = cum[:, length - 1 : length]
    tail = split3(jnp.exp(last - cum) * step)
    last = split3(jnp.broadcast_to(last, (heads, 128)))
    groups = nw // STATE
    width = nch // groups
    parts = pay_ref.shape[0]
    rows = STATE // parts
    his, los = [], []
    for g in range(groups):
        spread = spread_heads(g, heads, width)
        xt = (x_ref[:, g * width : (g + 1) * width].astype(F32) * to_lanes(tail, spread)).astype(BF16)
        state = dot_tn(w_ref[:, g * STATE : (g + 1) * STATE], xt).astype(BF16)
        pay_ref[:, g * rows : (g + 1) * rows, :] = state.reshape(parts, rows, width)
        total = to_lanes(last, spread)[0:1]
        high = total.astype(BF16).astype(F32)
        his.append(high)
        los.append(total - high)
    extra_rows = jnp.concatenate(his + los + [jnp.zeros((16 - 2 * groups, width), F32)], axis=0).astype(BF16)
    for p in range(parts):
        pay_ref[p, groups * rows :, :] = extra_rows
    for d in range(parts):
        block_refs[d][...] = pay_ref[jnp.bitwise_xor(place_ref[0], d)]


def within_kernel(x_ref, w_ref, r_ref, cum_ref, step_ref, direct_ref, y_ref):
    g = pl.program_id(0)
    heads, length = cum_ref.shape
    width = x_ref.shape[1]
    per = width // HEAD_DIM
    block = 128
    pick = iota((heads, 128), 0) == g * per + iota((heads, 128), 1)
    cols = to_lanes(split3(cum_ref[...]), pick.astype(F32))
    spread = spread_heads(g, heads, width)
    x = x_ref[...].astype(F32)
    xs = (x * to_lanes(split3(step_ref[...]), spread)).astype(BF16)
    direct = to_lanes(split3(jnp.broadcast_to(to_column(direct_ref[...]), (heads, 128))), spread)[0:1]
    first_half = iota((block, 128), 1) < HEAD_DIM
    causal = iota((block, block), 0) >= iota((block, block), 1)
    rows = [cum_ref[pl.ds(g * per + j, 1), :] for j in range(per)]
    for i in range(length // block):
        here = slice(i * block, (i + 1) * block)
        seen = (i + 1) * block
        gram = dot_nt(r_ref[here, :], w_ref[0:seen, :])
        outs = []
        for j in range(per):
            gap = cols[here, j : j + 1] - rows[j][:, 0:seen]
            edge = jnp.where(causal, gap[:, i * block :], -1e30)
            if i:
                gap = jnp.concatenate([gap[:, : i * block], edge], axis=1)
            else:
                gap = edge
            m = (gram * jnp.exp(gap)).astype(BF16)
            pair = (j // 2) * 128
            outs.append(dot(m, xs[0:seen, pair : pair + 128]))
        for q in range(per // 2):
            lanes = slice(q * 128, (q + 1) * 128)
            y_ref[here, lanes] = (
                jnp.where(first_half, outs[2 * q], outs[2 * q + 1]) + direct[:, lanes] * x[here, lanes]
            )


def plane_kernel(place_ref, *refs):
    *block_refs, before_ref, total_ref, z_ref = refs
    parts, height, width = z_ref.shape
    for d in range(parts):
        z_ref[jnp.bitwise_xor(place_ref[0], d)] = block_refs[d][...]
    groups = 4
    rows = (height - 16) // groups
    base = groups * rows
    his, los = [], []
    for g in range(groups):
        run = jnp.zeros((rows, width), F32)
        log = jnp.zeros((1, width), F32)
        here = slice(g * rows, (g + 1) * rows)
        for p in range(parts):
            before_ref[p, here, :] = run
            before_ref[p, base + g : base + g + 1, :] = log
            pad = z_ref[p, base : base + 16, :].astype(F32)
            own = pad[g : g + 1] + pad[groups + g : groups + g + 1]
            run = jnp.exp(own) * run + z_ref[p, here, :].astype(F32)
            log = log + own
        total_ref[here, :] = run.astype(BF16)
        high = log.astype(BF16).astype(F32)
        his.append(high)
        los.append(log - high)
    total_ref[base:, :] = jnp.concatenate(
        his + los + [jnp.zeros((16 - 2 * groups, width), F32)], axis=0
    ).astype(BF16)


def unpack_logs(ref, groups, base):
    pad = ref[base : base + 16, :].astype(F32)
    return pad[0:groups] + pad[groups : 2 * groups]


def double_kernel(later_ref, earlier_ref, out_ref):
    height, width = out_ref.shape
    groups = 4
    rows = (height - 16) // groups
    base = groups * rows
    later = unpack_logs(later_ref, groups, base)
    for g in range(groups):
        here = slice(g * rows, (g + 1) * rows)
        grown = jnp.exp(later[g : g + 1]) * earlier_ref[here, :].astype(F32)
        out_ref[here, :] = (grown + later_ref[here, :].astype(F32)).astype(BF16)
    total = later + unpack_logs(earlier_ref, groups, base)
    high = total.astype(BF16).astype(F32)
    out_ref[base:, :] = jnp.concatenate(
        [high, total - high, jnp.zeros((16 - 2 * groups, width), F32)], axis=0
    ).astype(BF16)


def enter_kernel(before_ref, later_ref, earlier_ref, out_ref):
    height, _ = later_ref.shape
    parts = before_ref.shape[0]
    groups = 4
    rows = (height - 16) // groups
    base = groups * rows
    later = unpack_logs(later_ref, groups, base)
    for g in range(groups):
        here = slice(g * rows, (g + 1) * rows)
        grown = jnp.exp(later[g : g + 1]) * earlier_ref[here, :].astype(F32)
        state = grown + later_ref[here, :].astype(F32)
        for p in range(parts):
            log = before_ref[p, base + g : base + g + 1, :]
            out_ref[p, here, :] = (before_ref[p, here, :] + jnp.exp(log) * state).astype(BF16)


def project_kernel(
    me_ref, y_ref, r_ref, s_ref, cum_ref, gate_ref, wo_ref,
    own_ref, up_ref, down_ref, opa_ref, opb_ref, natural_ref, gated_ref,
):
    heads, length = cum_ref.shape
    n = 4
    part = length // n
    groups = r_ref.shape[1] // STATE
    width = y_ref.shape[1] // groups

    @pl.when(pl.program_id(0) == 0)
    def _():
        me = me_ref[0]
        grown = split3(jnp.exp(cum_ref[...]))
        for g in range(groups):
            lanes = slice(g * width, (g + 1) * width)
            state = s_ref[:, g * 16 : (g + 1) * 16, :].reshape(STATE, width)
            carried = dot(r_ref[:, g * STATE : (g + 1) * STATE], state)
            y = y_ref[:, lanes] + to_lanes(grown, spread_heads(g, heads, width)) * carried
            natural_ref[:, lanes] = (y * silu(gate_ref[:, lanes].astype(F32))).astype(BF16)
        for k in range(n):
            rows = pl.ds(pl.multiple_of(lax.rem(me + k, n) * part, part), part)
            gated_ref[k * part : (k + 1) * part, :] = natural_ref[rows, :]

    out = dot(gated_ref[...], wo_ref[...]).astype(BF16)
    own_ref[...] = out[0:part]
    up_ref[...] = out[part : 2 * part]
    opa_ref[...] = out[2 * part : 2 * part + part // 2]
    opb_ref[...] = out[2 * part + part // 2 : 3 * part]
    down_ref[...] = out[3 * part : 4 * part]


def norm_kernel(own_ref, u_ref, d_ref, gain_ref, out_ref):
    total = own_ref[...].astype(F32) + u_ref[...].astype(F32) + d_ref[...].astype(F32)
    mean = jnp.mean(total * total, axis=-1, keepdims=True)
    out_ref[...] = (total * lax.rsqrt(mean + EPS) * gain_ref[...]).astype(BF16)


def dispatch_kernel(
    me_ref, tok_ref, gain_ref, routes_ref, ch_ref, wr_ref, rd_ref, out_ref, dest_ref, edge_ref, normed_ref
):
    count = tok_ref.shape[0]
    slots, quarter = out_ref.shape
    experts = slots // CAP
    nch, nw = ch_ref.shape[1], wr_ref.shape[1]
    edge_ref[:, 0:nch] = ch_ref[...]
    edge_ref[:, nch : nch + nw] = wr_ref[...]
    edge_ref[:, nch + nw :] = rd_ref[...]
    v = tok_ref[...].astype(F32)
    mean = jnp.mean(v * v, axis=-1, keepdims=True)
    normed_ref[...] = (v * lax.rsqrt(mean + EPS) * gain_ref[...]).astype(BF16)
    ids = iota((experts, count), 0)
    is_first, is_second = ids == routes_ref[0:1, :], ids == routes_ref[1:2, :]
    named = jnp.where(is_first | is_second, 1.0, 0.0).astype(BF16)
    before = jnp.where(iota((count, count), 0) < iota((count, count), 1), 1.0, 0.0).astype(BF16)
    place = dot(named, before) + (ids * CAP).astype(F32)
    dest0 = jnp.sum(jnp.where(is_first, place, 0.0), axis=0, keepdims=True).astype(jnp.int32)
    dest1 = jnp.sum(jnp.where(is_second, place, 0.0), axis=0, keepdims=True).astype(jnp.int32)
    dest_ref[0:1, :] = dest0
    dest_ref[1:2, :] = dest1
    slot = iota((slots, count), 0)
    chosen = jnp.where((slot == dest0) | (slot == dest1), 1.0, 0.0).astype(BF16)
    lanes = pl.ds(pl.multiple_of(me_ref[0] * quarter, quarter), quarter)
    out_ref[...] = dot(chosen, normed_ref[:, lanes]).astype(BF16)


def combine_kernel(back_ref, dest_ref, weight_ref, out_ref):
    count = dest_ref.shape[1]
    slot = iota((back_ref.shape[0], count), 0)
    mix = jnp.where(slot == dest_ref[0:1, :], weight_ref[0:1, :], 0.0) + jnp.where(
        slot == dest_ref[1:2, :], weight_ref[1:2, :], 0.0
    )
    high = mix.astype(BF16)
    low = (mix - high.astype(F32)).astype(BF16)
    back = back_ref[...]
    out_ref[...] = (dot_tn(high, back) + dot_tn(low, back)).astype(BF16)


def hidden_kernel(me_ref, own, left, right, op0, op1, gate_ref, up_ref, out_ref):
    me = me_ref[0]
    size = own.shape[1]
    opposite = jnp.where(pl.program_id(0) < pl.num_programs(0) // 2, op0[...], op1[...])

    def product(w):
        def rows(shift):
            return pl.ds(pl.multiple_of(lax.rem(me + shift, 4) * size, size), size)

        total = dot(own[...], w[rows(0), :]) + dot(left[...], w[rows(3), :])
        return total + dot(right[...], w[rows(1), :]) + dot(opposite, w[rows(2), :])

    out_ref[...] = (silu(product(gate_ref)) * product(up_ref)).astype(BF16)


def result_kernel(me_ref, own, left, right, op0, op1, down_own, down_left, down_right, down_cross, out_ref):
    opposite = jnp.where(pl.program_id(0) < pl.num_programs(0) // 2, op0[...], op1[...])
    total = dot(own[...], down_own[...]) + dot(left[...], down_left[...])
    total = total + dot(right[...], down_right[...]) + dot(opposite, down_cross[...])
    out_ref[...] = total.astype(BF16)


def ring_pieces(x, axis):
    n = lax.axis_size(axis)
    plus = [(i, (i + 1) % n) for i in range(n)]
    minus = [(i, (i - 1) % n) for i in range(n)]
    half = x.shape[0] // 2
    left = lax.ppermute(x, axis, plus)
    right = lax.ppermute(x, axis, minus)
    op0 = lax.ppermute(left[:half], axis, plus)
    op1 = lax.ppermute(right[half:], axis, minus)
    return x, left, right, op0, op1


def ring_call(kernel, me, pieces, weights, columns, tile):
    rows = pieces[0].shape[0]
    steps = rows // tile
    smem = pl.BlockSpec(memory_space=pltpu.SMEM)
    specs = [smem]
    specs += [pl.BlockSpec((tile, p.shape[1]), lambda i: (i, 0)) for p in pieces[:3]]
    specs.append(pl.BlockSpec((tile, pieces[3].shape[1]), lambda i: (jnp.minimum(i, steps // 2 - 1), 0)))
    specs.append(pl.BlockSpec((tile, pieces[4].shape[1]), lambda i: (jnp.maximum(i - steps // 2, 0), 0)))
    specs += [pl.BlockSpec(w.shape, lambda i: (0, 0)) for w in weights]
    depth = sum(w.shape[0] for w in weights)
    return pl.pallas_call(
        kernel,
        grid=(steps,),
        in_specs=specs,
        out_specs=pl.BlockSpec((tile, columns), lambda i: (i, 0)),
        out_shape=jax.ShapeDtypeStruct((rows, columns), BF16),
        compiler_params=params(MID),
        cost_estimate=cost(2 * rows * depth * columns, rows * depth * 2),
    )(me, *pieces, *weights)


def per_device(
    mixer_channels_raw,
    write_vectors_raw,
    read_vectors_raw,
    gate_logits,
    step_size_raw,
    extra_log_decay,
    mixer_conv_taps,
    write_conv_taps,
    read_conv_taps,
    step_size_bias,
    log_decay_rate,
    direct_path_weight,
    mixer_output_weight,
    mixer_norm_scale,
    routed_tokens,
    expert_norm_scale,
    routes,
    routing_weights,
    expert_gate_matrix,
    expert_up_matrix,
    expert_down_matrix,
):
    sds = jax.ShapeDtypeStruct
    smem = pl.BlockSpec(memory_space=pltpu.SMEM)
    tp = lax.axis_index("tp")
    me = tp.reshape(1).astype(jnp.int32)
    tps = lax.axis_size("tp")
    plus = [(i, (i + 1) % tps) for i in range(tps)]
    minus = [(i, (i - 1) % tps) for i in range(tps)]
    cross = [(i, (i + 2) % tps) for i in range(tps)]

    tokens, model = routed_tokens.shape
    experts = lax.axis_size(EP)
    slots = experts * CAP
    quarter = model // tps
    length, channels = mixer_channels_raw.shape
    nw = write_vectors_raw.shape[1]
    last_rows = lambda a: pl.BlockSpec((16, a.shape[1]), lambda i: (a.shape[0] // 16 - 1, 0))
    entire = lambda shape: pl.BlockSpec(shape, lambda i: (0,) * len(shape))
    outgoing, dest, edge = pl.pallas_call(
        dispatch_kernel,
        grid=(1,),
        in_specs=[smem, entire((tokens, model)), entire((1, model)), entire((2, tokens))]
        + [last_rows(a) for a in (mixer_channels_raw, write_vectors_raw, read_vectors_raw)],
        out_specs=[entire((slots, quarter)), entire((2, tokens)), entire((16, channels + 2 * nw))],
        out_shape=(
            sds((slots, quarter), BF16),
            sds((2, tokens), jnp.int32),
            sds((16, channels + 2 * nw), BF16),
        ),
        scratch_shapes=[pltpu.VMEM((tokens, model), BF16)],
        compiler_params=params(BIG),
        cost_estimate=cost(2 * slots * tokens * quarter, 4 * MIB),
        name="dispatch",
    )(
        me,
        routed_tokens,
        expert_norm_scale[None, :],
        routes.T,
        mixer_channels_raw,
        write_vectors_raw,
        read_vectors_raw,
    )
    arrived = lax.all_to_all(
        outgoing.reshape(experts, CAP, quarter), EP, split_axis=0, concat_axis=0, tiled=True
    )
    arrived = arrived.reshape(slots, quarter)

    ff = expert_down_matrix.shape[1]
    down = expert_down_matrix[0]

    def feature_block(shift):
        return lax.dynamic_slice(down, (0, lax.rem(tp + shift, tps) * quarter), (ff, quarter))

    d_own = feature_block(0)
    d_left = lax.ppermute(feature_block(1), "tp", plus)
    d_right = lax.ppermute(feature_block(3), "tp", minus)
    d_cross = lax.ppermute(feature_block(2), "tp", cross)

    heads = step_size_raw.shape[1]
    groups = nw // STATE
    width = channels // groups
    edge = lax.ppermute(edge, EP, [(i, i + 1) for i in range(experts - 1)])
    place = lax.axis_index(PLANE).reshape(1).astype(jnp.int32)
    parts = lax.axis_size(PLANE)
    height = groups * (STATE // parts) + 16
    x, w, r, cum, step, *blocks = pl.pallas_call(
        conv_kernel,
        in_specs=[smem] + vmem(11),
        out_specs=vmem(5 + parts),
        out_shape=(
            sds((length, channels), BF16),
            sds((length, nw), BF16),
            sds((length, nw), BF16),
            sds((heads, length), F32),
            sds((heads, length), F32),
        )
        + (sds((height, width), BF16),) * parts,
        scratch_shapes=[pltpu.VMEM((parts, height, width), BF16)],
        compiler_params=params(BIG),
        cost_estimate=cost(2 * length * STATE * channels * 8, 4 * MIB),
        name="conv",
    )(
        place,
        mixer_channels_raw,
        write_vectors_raw,
        read_vectors_raw,
        edge,
        mixer_conv_taps,
        write_conv_taps,
        read_conv_taps,
        step_size_raw.T,
        extra_log_decay.T,
        step_size_bias[None, :],
        log_decay_rate[None, :],
    )
    for d in range(1, parts):
        blocks[d] = lax.ppermute(blocks[d], PLANE, [(i, i ^ d) for i in range(parts)])
    before, total = pl.pallas_call(
        plane_kernel,
        in_specs=[smem] + vmem(parts),
        out_specs=vmem(2),
        out_shape=(sds((parts, height, width), F32), sds((height, width), BF16)),
        scratch_shapes=[pltpu.VMEM((parts, height, width), BF16)],
        compiler_params=params(MID),
        cost_estimate=cost(1000000, MIB),
        name="plane",
    )(place, *blocks)
    planes = lax.axis_size("ep_0")

    def from_below(value, shift):
        return lax.ppermute(value, "ep_0", [(i, i + shift) for i in range(planes - shift)])

    later = from_below(total, 1)
    shift = 1
    while 2 * shift < planes:
        earlier = from_below(later, shift)
        later = pl.pallas_call(
            double_kernel,
            in_specs=vmem(2),
            out_specs=vmem(1)[0],
            out_shape=sds((height, width), BF16),
            compiler_params=params(MID),
            cost_estimate=cost(200000, MIB // 8),
            name="double",
        )(later, earlier)
        shift *= 2
    earlier = from_below(later, shift)
    entering = pl.pallas_call(
        enter_kernel,
        in_specs=vmem(3),
        out_specs=vmem(1)[0],
        out_shape=sds((parts, height - 16, width), BF16),
        compiler_params=params(MID),
        cost_estimate=cost(1000000, MIB),
        name="enter",
    )(before, later, earlier)
    entering = lax.all_to_all(entering, PLANE, 0, 0, tiled=True)

    y = pl.pallas_call(
        within_kernel,
        grid=(groups,),
        in_specs=[
            pl.BlockSpec((length, width), lambda g: (0, g)),
            pl.BlockSpec((length, STATE), lambda g: (0, g)),
            pl.BlockSpec((length, STATE), lambda g: (0, g)),
            pl.BlockSpec((heads, length), lambda g: (0, 0)),
            pl.BlockSpec((heads, length), lambda g: (0, 0)),
            pl.BlockSpec((1, heads), lambda g: (0, 0)),
        ],
        out_specs=pl.BlockSpec((length, width), lambda g: (0, g)),
        out_shape=sds((length, channels), F32),
        compiler_params=params(BIG),
        cost_estimate=cost(4 * length * length * channels, 4 * MIB),
        name="within",
    )(x, w, r, cum, step, direct_path_weight[None, :])

    out_dim = mixer_output_weight.shape[1]
    part = length // tps
    tile = 512
    row_block = lambda rows: pl.BlockSpec((rows, tile), lambda j: (0, j))
    whole = lambda a: pl.BlockSpec(a.shape, lambda j: (0,) * a.ndim)
    own, up, dn, opa, opb = pl.pallas_call(
        project_kernel,
        grid=(out_dim // tile,),
        in_specs=[smem]
        + [whole(a) for a in (y, r, entering, cum, gate_logits)]
        + [pl.BlockSpec((channels, tile), lambda j: (0, j))],
        out_specs=(row_block(part), row_block(part), row_block(part), row_block(part // 2), row_block(part // 2)),
        out_shape=(
            sds((part, out_dim), BF16),
            sds((part, out_dim), BF16),
            sds((part, out_dim), BF16),
            sds((part // 2, out_dim), BF16),
            sds((part // 2, out_dim), BF16),
        ),
        scratch_shapes=[pltpu.VMEM((length, channels), BF16)] * 2,
        compiler_params=params(MID),
        cost_estimate=cost(2 * length * channels * out_dim, 6 * MIB),
        name="project",
    )(me, y, r, entering, cum, gate_logits, mixer_output_weight)
    opa = lax.ppermute(opa, "tp", plus)
    opb = lax.ppermute(opb, "tp", minus)
    half = part // 2
    up = jnp.concatenate([(up[:half].astype(F32) + opa.astype(F32)).astype(BF16), up[half:]], axis=0)
    dn = jnp.concatenate([dn[:half], (dn[half:].astype(F32) + opb.astype(F32)).astype(BF16)], axis=0)
    up = lax.ppermute(up, "tp", plus)
    dn = lax.ppermute(dn, "tp", minus)
    mixer_out = pl.pallas_call(
        norm_kernel,
        in_specs=vmem(4),
        out_specs=vmem(1)[0],
        out_shape=sds((part, out_dim), BF16),
        compiler_params=params(MID),
        cost_estimate=cost(1000000, 2 * MIB),
        name="norm",
    )(own, up, dn, mixer_norm_scale[None, :])

    pieces = ring_pieces(arrived, "tp")
    hidden = ring_call(hidden_kernel, me, pieces, (expert_gate_matrix[0], expert_up_matrix[0]), ff, 512)
    pieces = ring_pieces(hidden, "tp")
    result = ring_call(result_kernel, me, pieces, (d_own, d_left, d_right, d_cross), quarter, 512)
    returned = lax.all_to_all(
        result.reshape(experts, CAP, quarter), EP, split_axis=0, concat_axis=0, tiled=True
    )
    returned = returned.reshape(slots, quarter)
    expert_out = pl.pallas_call(
        combine_kernel,
        in_specs=vmem(3),
        out_specs=vmem(1)[0],
        out_shape=sds((tokens, quarter), BF16),
        compiler_params=params(MID),
        cost_estimate=cost(4 * slots * tokens * quarter, 2 * MIB),
        name="combine",
    )(returned, dest, routing_weights.T)
    return (mixer_out, expert_out)


def solution(mesh):
    split = Mesh(mesh.devices.reshape(8, 4, 2, mesh.shape["tp"]), EP_TP)
    placed = (
        P(EP, "tp"),
        P(EP, "tp"),
        P(EP, "tp"),
        P(EP, "tp"),
        P(EP, "tp"),
        P(EP, "tp"),
        P(None, "tp"),
        P(None, "tp"),
        P(None, "tp"),
        P("tp"),
        P("tp"),
        P("tp"),
        P("tp", None),
        P(),
        P(EP, None),
        P(),
        P(EP, None),
        P(EP, None),
        P(EP, None, "tp"),
        P(EP, None, "tp"),
        P(EP, "tp", None),
    )

    return jax.shard_map(
        per_device,
        mesh=split,
        in_specs=placed,
        out_specs=(P(EP_TP, None), P(EP, "tp")),
        check_vma=False,
    )
```

```python
import jax
import jax.numpy as jnp
from jax import lax
from jax.experimental import pallas as pl
from jax.experimental.pallas import tpu as pltpu
from jax.sharding import Mesh
from jax.sharding import PartitionSpec as P


HEAD_DIM = 64
STATE = 128
CAP = 16
EP = ("ep_0", "ep_1", "ep_2")
PLANE = ("ep_1", "ep_2")
EP_TP = ("ep_0", "ep_1", "ep_2", "tp")
EPS = 1e-06
F32 = jnp.float32
BF16 = jnp.bfloat16
MIB = 1024 * 1024
BIG = 56
MID = 24


def vmem(count):
    return [pl.BlockSpec(memory_space=pltpu.VMEM)] * count


def params(mib):
    return pltpu.CompilerParams(vmem_limit_bytes=mib * MIB)


def cost(flops, nbytes):
    return pl.CostEstimate(flops=flops, bytes_accessed=nbytes, transcendentals=0)


def iota(shape, dim):
    return lax.broadcasted_iota(jnp.int32, shape, dim)


def spread_heads(group, heads, width):
    per = width // HEAD_DIM
    return (iota((heads, width), 0) == group * per + iota((heads, width), 1) // HEAD_DIM).astype(F32)


def dot(a, b, precision=None):
    return jnp.dot(a, b, preferred_element_type=F32, precision=precision)


def dot_tn(a, b):
    return lax.dot_general(a, b, (((0,), (0,)), ((), ())), preferred_element_type=F32)


def dot_nt(a, b):
    return lax.dot_general(a, b, (((1,), (1,)), ((), ())), preferred_element_type=F32)


def silu(x):
    return 0.5 * x * (1.0 + jnp.tanh(0.5 * x))


def split3(x):
    high = x.astype(BF16)
    rest = x - high.astype(F32)
    middle = rest.astype(BF16)
    low = (rest - middle.astype(F32)).astype(BF16)
    return jnp.concatenate([high, middle, low], axis=0)


def to_lanes(terms, mask):
    return dot_tn(terms, jnp.concatenate([mask.astype(BF16)] * 3, axis=0))


def to_column(row):
    n = row.shape[1]
    return jnp.sum(jnp.where(iota((n, n), 0) == iota((n, n), 1), row, 0.0), axis=1, keepdims=True)


def conv_kernel(
    place_ref, ch_ref, wr_ref, rd_ref, edge_ref, ct_ref, wt_ref, rt_ref, sraw_ref, extra_ref, bias_ref, rate_ref,
    x_ref, w_ref, r_ref, cum_ref, step_ref, *rest,
):
    *block_refs, pay_ref = rest
    heads, length = sraw_ref.shape
    tile = 128

    def conv(src, taps, dst, first):
        def body(i, carry):
            lanes = pl.ds(pl.multiple_of(i * tile, tile), tile)
            edges = edge_ref[:, pl.ds(pl.multiple_of(first + i * tile, tile), tile)].astype(F32)
            joined = jnp.concatenate([edges[8:16], src[:, lanes].astype(F32)], axis=0)
            t = taps[:, lanes]
            total = t[0:1] * joined[5 : 5 + length]
            for k in range(1, t.shape[0]):
                total = total + t[k : k + 1] * joined[5 + k : 5 + k + length]
            dst[:, lanes] = silu(total).astype(BF16)
            return carry

        lax.fori_loop(0, src.shape[1] // tile, body, 0)

    nch, nw = ch_ref.shape[1], wr_ref.shape[1]
    conv(ch_ref, ct_ref, x_ref, 0)
    conv(wr_ref, wt_ref, w_ref, nch)
    conv(rd_ref, rt_ref, r_ref, nch + nw)

    raw = sraw_ref[...].astype(F32) + to_column(bias_ref[...])
    step = jnp.maximum(raw, 0.0) + jnp.log1p(jnp.exp(-jnp.abs(raw)))
    decay = extra_ref[...] - step * to_column(jnp.exp(rate_ref[...]))
    upto = jnp.where(iota((length, length), 0) <= iota((length, length), 1), 1.0, 0.0).astype(BF16)
    sums = dot(split3(decay), upto)
    cum = sums[0:heads] + sums[heads : 2 * heads] + sums[2 * heads :]
    cum_ref[...] = cum
    step_ref[...] = step
    last = cum[:, length - 1 : length]
    tail = split3(jnp.exp(last - cum) * step)
    last = split3(jnp.broadcast_to(last, (heads, 128)))
    groups = nw // STATE
    width = nch // groups
    parts = pay_ref.shape[0]
    rows = STATE // parts
    his, los = [], []
    for g in range(groups):
        spread = spread_heads(g, heads, width)
        xt = (x_ref[:, g * width : (g + 1) * width].astype(F32) * to_lanes(tail, spread)).astype(BF16)
        state = dot_tn(w_ref[:, g * STATE : (g + 1) * STATE], xt).astype(BF16)
        pay_ref[:, g * rows : (g + 1) * rows, :] = state.reshape(parts, rows, width)
        total = to_lanes(last, spread)[0:1]
        high = total.astype(BF16).astype(F32)
        his.append(high)
        los.append(total - high)
    extra_rows = jnp.concatenate(his + los + [jnp.zeros((16 - 2 * groups, width), F32)], axis=0).astype(BF16)
    for p in range(parts):
        pay_ref[p, groups * rows :, :] = extra_rows
    for d in range(parts):
        block_refs[d][...] = pay_ref[jnp.bitwise_xor(place_ref[0], d)]


def within_kernel(x_ref, w_ref, r_ref, cum_ref, step_ref, direct_ref, y_ref):
    g = pl.program_id(0)
    heads, length = cum_ref.shape
    width = x_ref.shape[1]
    per = width // HEAD_DIM
    block = 128
    pick = iota((heads, 128), 0) == g * per + iota((heads, 128), 1)
    cols = to_lanes(split3(cum_ref[...]), pick.astype(F32))
    spread = spread_heads(g, heads, width)
    x = x_ref[...].astype(F32)
    xs = (x * to_lanes(split3(step_ref[...]), spread)).astype(BF16)
    direct = to_lanes(split3(jnp.broadcast_to(to_column(direct_ref[...]), (heads, 128))), spread)[0:1]
    first_half = iota((block, 128), 1) < HEAD_DIM
    causal = iota((block, block), 0) >= iota((block, block), 1)
    rows = [cum_ref[pl.ds(g * per + j, 1), :] for j in range(per)]
    for i in range(length // block):
        here = slice(i * block, (i + 1) * block)
        seen = (i + 1) * block
        gram = dot_nt(r_ref[here, :], w_ref[0:seen, :])
        outs = []
        for j in range(per):
            gap = cols[here, j : j + 1] - rows[j][:, 0:seen]
            edge = jnp.where(causal, gap[:, i * block :], -1e30)
            if i:
                gap = jnp.concatenate([gap[:, : i * block], edge], axis=1)
            else:
                gap = edge
            m = (gram * jnp.exp(gap)).astype(BF16)
            pair = (j // 2) * 128
            outs.append(dot(m, xs[0:seen, pair : pair + 128]))
        for q in range(per // 2):
            lanes = slice(q * 128, (q + 1) * 128)
            y_ref[here, lanes] = (
                jnp.where(first_half, outs[2 * q], outs[2 * q + 1]) + direct[:, lanes] * x[here, lanes]
            )


def plane_kernel(place_ref, *refs):
    *block_refs, before_ref, total_ref, z_ref = refs
    parts, height, width = z_ref.shape
    for d in range(parts):
        z_ref[jnp.bitwise_xor(place_ref[0], d)] = block_refs[d][...]
    groups = 4
    rows = (height - 16) // groups
    base = groups * rows
    his, los = [], []
    for g in range(groups):
        run = jnp.zeros((rows, width), F32)
        log = jnp.zeros((1, width), F32)
        here = slice(g * rows, (g + 1) * rows)
        for p in range(parts):
            before_ref[p, here, :] = run
            before_ref[p, base + g : base + g + 1, :] = log
            pad = z_ref[p, base : base + 16, :].astype(F32)
            own = pad[g : g + 1] + pad[groups + g : groups + g + 1]
            run = jnp.exp(own) * run + z_ref[p, here, :].astype(F32)
            log = log + own
        total_ref[here, :] = run.astype(BF16)
        high = log.astype(BF16).astype(F32)
        his.append(high)
        los.append(log - high)
    total_ref[base:, :] = jnp.concatenate(
        his + los + [jnp.zeros((16 - 2 * groups, width), F32)], axis=0
    ).astype(BF16)


def unpack_logs(ref, groups, base):
    pad = ref[base : base + 16, :].astype(F32)
    return pad[0:groups] + pad[groups : 2 * groups]


def enter_kernel(zi_ref, before_ref, planes_ref, out_ref):
    count, height, width = planes_ref.shape
    parts = before_ref.shape[0]
    groups = 4
    rows = (height - 16) // groups
    base = groups * rows
    mine = zi_ref[0]
    logs = [unpack_logs(planes_ref.at[k], groups, base) for k in range(count)]
    for g in range(groups):
        here = slice(g * rows, (g + 1) * rows)
        state = jnp.zeros((rows, width), F32)
        for k in range(count - 1):
            new = jnp.exp(logs[k][g : g + 1]) * state + planes_ref[k, here, :].astype(F32)
            state = jnp.where(k < mine, new, state)
        for p in range(parts):
            log = before_ref[p, base + g : base + g + 1, :]
            out_ref[p, here, :] = (before_ref[p, here, :] + jnp.exp(log) * state).astype(BF16)


def project_kernel(
    me_ref, y_ref, r_ref, s_ref, cum_ref, gate_ref, wo_ref,
    own_ref, up_ref, down_ref, opa_ref, opb_ref, natural_ref, gated_ref,
):
    heads, length = cum_ref.shape
    n = 4
    part = length // n
    groups = r_ref.shape[1] // STATE
    width = y_ref.shape[1] // groups

    @pl.when(pl.program_id(0) == 0)
    def _():
        me = me_ref[0]
        grown = split3(jnp.exp(cum_ref[...]))
        for g in range(groups):
            lanes = slice(g * width, (g + 1) * width)
            state = s_ref[:, g * 16 : (g + 1) * 16, :].reshape(STATE, width)
            carried = dot(r_ref[:, g * STATE : (g + 1) * STATE], state)
            y = y_ref[:, lanes] + to_lanes(grown, spread_heads(g, heads, width)) * carried
            natural_ref[:, lanes] = (y * silu(gate_ref[:, lanes].astype(F32))).astype(BF16)
        for k in range(n):
            rows = pl.ds(pl.multiple_of(lax.rem(me + k, n) * part, part), part)
            gated_ref[k * part : (k + 1) * part, :] = natural_ref[rows, :]

    out = dot(gated_ref[...], wo_ref[...]).astype(BF16)
    own_ref[...] = out[0:part]
    up_ref[...] = out[part : 2 * part]
    opa_ref[...] = out[2 * part : 2 * part + part // 2]
    opb_ref[...] = out[2 * part + part // 2 : 3 * part]
    down_ref[...] = out[3 * part : 4 * part]


def norm_kernel(own_ref, u_ref, d_ref, gain_ref, out_ref):
    total = own_ref[...].astype(F32) + u_ref[...].astype(F32) + d_ref[...].astype(F32)
    mean = jnp.mean(total * total, axis=-1, keepdims=True)
    out_ref[...] = (total * lax.rsqrt(mean + EPS) * gain_ref[...]).astype(BF16)


def dispatch_kernel(
    me_ref, tok_ref, gain_ref, routes_ref, ch_ref, wr_ref, rd_ref, out_ref, dest_ref, edge_ref, normed_ref
):
    count = tok_ref.shape[0]
    slots, quarter = out_ref.shape
    experts = slots // CAP
    nch, nw = ch_ref.shape[1], wr_ref.shape[1]
    edge_ref[:, 0:nch] = ch_ref[...]
    edge_ref[:, nch : nch + nw] = wr_ref[...]
    edge_ref[:, nch + nw :] = rd_ref[...]
    v = tok_ref[...].astype(F32)
    mean = jnp.mean(v * v, axis=-1, keepdims=True)
    normed_ref[...] = (v * lax.rsqrt(mean + EPS) * gain_ref[...]).astype(BF16)
    ids = iota((experts, count), 0)
    is_first, is_second = ids == routes_ref[0:1, :], ids == routes_ref[1:2, :]
    named = jnp.where(is_first | is_second, 1.0, 0.0).astype(BF16)
    before = jnp.where(iota((count, count), 0) < iota((count, count), 1), 1.0, 0.0).astype(BF16)
    place = dot(named, before) + (ids * CAP).astype(F32)
    dest0 = jnp.sum(jnp.where(is_first, place, 0.0), axis=0, keepdims=True).astype(jnp.int32)
    dest1 = jnp.sum(jnp.where(is_second, place, 0.0), axis=0, keepdims=True).astype(jnp.int32)
    dest_ref[0:1, :] = dest0
    dest_ref[1:2, :] = dest1
    slot = iota((slots, count), 0)
    chosen = jnp.where((slot == dest0) | (slot == dest1), 1.0, 0.0).astype(BF16)
    lanes = pl.ds(pl.multiple_of(me_ref[0] * quarter, quarter), quarter)
    out_ref[...] = dot(chosen, normed_ref[:, lanes]).astype(BF16)


def combine_kernel(back_ref, dest_ref, weight_ref, out_ref):
    count = dest_ref.shape[1]
    slot = iota((back_ref.shape[0], count), 0)
    mix = jnp.where(slot == dest_ref[0:1, :], weight_ref[0:1, :], 0.0) + jnp.where(
        slot == dest_ref[1:2, :], weight_ref[1:2, :], 0.0
    )
    high = mix.astype(BF16)
    low = (mix - high.astype(F32)).astype(BF16)
    back = back_ref[...]
    out_ref[...] = (dot_tn(high, back) + dot_tn(low, back)).astype(BF16)


def tp_rows(me, shift, size):
    return pl.ds(pl.multiple_of(lax.rem(me + shift, 4) * size, size), size)


def hidden_near_kernel(me_ref, own, left0, left1, right0, right1, gate_ref, up_ref, out_ref):
    half, size = left0.shape
    columns = gate_ref.shape[1]
    for c, (left, right) in enumerate(((left0, right0), (left1, right1))):
        here = slice(c * half, (c + 1) * half)
        for k, w in enumerate((gate_ref, up_ref)):
            total = dot(own[here, :], w[tp_rows(me_ref[0], 0, size), :])
            total = total + dot(left[...], w[tp_rows(me_ref[0], 3, size), :])
            total = total + dot(right[...], w[tp_rows(me_ref[0], 1, size), :])
            out_ref[here, k * columns : (k + 1) * columns] = total


def hidden_kernel(me_ref, near_ref, op0, op1, gate_ref, up_ref, out0_ref, out1_ref):
    half, size = op0.shape
    columns = gate_ref.shape[1]
    for c, (op, out_ref) in enumerate(((op0, out0_ref), (op1, out1_ref))):
        here = slice(c * half, (c + 1) * half)
        rows = tp_rows(me_ref[0], 2, size)
        gate = near_ref[here, :columns] + dot(op[...], gate_ref[rows, :])
        up = near_ref[here, columns:] + dot(op[...], up_ref[rows, :])
        out_ref[...] = (silu(gate) * up).astype(BF16)


def result_near_kernel(own0, own1, left0, left1, right0, right1, down_own, down_left, down_right, out_ref):
    half = own0.shape[0]
    for c, (own, left, right) in enumerate(((own0, left0, right0), (own1, left1, right1))):
        total = dot(own[...], down_own[...]) + dot(left[...], down_left[...])
        out_ref[c * half : (c + 1) * half, :] = total + dot(right[...], down_right[...])


def result_kernel(near_ref, op0, op1, down_ref, out_ref):
    half = op0.shape[0]
    for c, op in enumerate((op0, op1)):
        here = slice(c * half, (c + 1) * half)
        out_ref[here, :] = (near_ref[here, :] + dot(op[...], down_ref[...])).astype(BF16)


def ring_step(x, axis, by):
    n = lax.axis_size(axis)
    return lax.ppermute(x, axis, [(i, (i + by) % n) for i in range(n)])


def ring(first, second, axis):
    left0 = ring_step(first, axis, 1)
    right1 = ring_step(second, axis, -1)
    left1 = ring_step(second, axis, 1)
    right0 = ring_step(first, axis, -1)
    op0 = ring_step(left0, axis, 1)
    op1 = ring_step(right1, axis, -1)
    return left0, left1, right0, right1, op0, op1


def expert_call(kernel, scalars, arrays, shapes, flops, grant=MID):
    return pl.pallas_call(
        kernel,
        in_specs=[pl.BlockSpec(memory_space=pltpu.SMEM)] * len(scalars) + vmem(len(arrays)),
        out_specs=vmem(len(shapes)),
        out_shape=shapes,
        compiler_params=params(grant),
        cost_estimate=cost(flops, 4 * MIB),
    )(*scalars, *arrays)


def per_device(
    mixer_channels_raw,
    write_vectors_raw,
    read_vectors_raw,
    gate_logits,
    step_size_raw,
    extra_log_decay,
    mixer_conv_taps,
    write_conv_taps,
    read_conv_taps,
    step_size_bias,
    log_decay_rate,
    direct_path_weight,
    mixer_output_weight,
    mixer_norm_scale,
    routed_tokens,
    expert_norm_scale,
    routes,
    routing_weights,
    expert_gate_matrix,
    expert_up_matrix,
    expert_down_matrix,
):
    sds = jax.ShapeDtypeStruct
    smem = pl.BlockSpec(memory_space=pltpu.SMEM)
    tp = lax.axis_index("tp")
    me = tp.reshape(1).astype(jnp.int32)
    tps = lax.axis_size("tp")
    plus = [(i, (i + 1) % tps) for i in range(tps)]
    minus = [(i, (i - 1) % tps) for i in range(tps)]
    cross = [(i, (i + 2) % tps) for i in range(tps)]

    tokens, model = routed_tokens.shape
    experts = lax.axis_size(EP)
    slots = experts * CAP
    quarter = model // tps
    length, channels = mixer_channels_raw.shape
    nw = write_vectors_raw.shape[1]
    last_rows = lambda a: pl.BlockSpec((16, a.shape[1]), lambda i: (a.shape[0] // 16 - 1, 0))
    entire = lambda shape: pl.BlockSpec(shape, lambda i: (0,) * len(shape))
    outgoing, dest, edge = pl.pallas_call(
        dispatch_kernel,
        grid=(1,),
        in_specs=[smem, entire((tokens, model)), entire((1, model)), entire((2, tokens))]
        + [last_rows(a) for a in (mixer_channels_raw, write_vectors_raw, read_vectors_raw)],
        out_specs=[entire((slots, quarter)), entire((2, tokens)), entire((16, channels + 2 * nw))],
        out_shape=(
            sds((slots, quarter), BF16),
            sds((2, tokens), jnp.int32),
            sds((16, channels + 2 * nw), BF16),
        ),
        scratch_shapes=[pltpu.VMEM((tokens, model), BF16)],
        compiler_params=params(BIG),
        cost_estimate=cost(2 * slots * tokens * quarter, 4 * MIB),
        name="dispatch",
    )(
        me,
        routed_tokens,
        expert_norm_scale[None, :],
        routes.T,
        mixer_channels_raw,
        write_vectors_raw,
        read_vectors_raw,
    )
    arrived = lax.all_to_all(
        outgoing.reshape(experts, CAP, quarter), EP, split_axis=0, concat_axis=0, tiled=True
    )
    arrived = arrived.reshape(slots, quarter)

    ff = expert_down_matrix.shape[1]
    down = expert_down_matrix[0]

    def feature_block(shift):
        return lax.dynamic_slice(down, (0, lax.rem(tp + shift, tps) * quarter), (ff, quarter))

    d_own = feature_block(0)
    d_left = lax.ppermute(feature_block(1), "tp", plus)
    d_right = lax.ppermute(feature_block(3), "tp", minus)
    d_cross = lax.ppermute(feature_block(2), "tp", cross)

    heads = step_size_raw.shape[1]
    groups = nw // STATE
    width = channels // groups
    edge = lax.ppermute(edge, EP, [(i, i + 1) for i in range(experts - 1)])
    place = lax.axis_index(PLANE).reshape(1).astype(jnp.int32)
    parts = lax.axis_size(PLANE)
    height = groups * (STATE // parts) + 16
    x, w, r, cum, step, *blocks = pl.pallas_call(
        conv_kernel,
        in_specs=[smem] + vmem(11),
        out_specs=vmem(5 + parts),
        out_shape=(
            sds((length, channels), BF16),
            sds((length, nw), BF16),
            sds((length, nw), BF16),
            sds((heads, length), F32),
            sds((heads, length), F32),
        )
        + (sds((height, width), BF16),) * parts,
        scratch_shapes=[pltpu.VMEM((parts, height, width), BF16)],
        compiler_params=params(BIG),
        cost_estimate=cost(2 * length * STATE * channels * 8, 4 * MIB),
        name="conv",
    )(
        place,
        mixer_channels_raw,
        write_vectors_raw,
        read_vectors_raw,
        edge,
        mixer_conv_taps,
        write_conv_taps,
        read_conv_taps,
        step_size_raw.T,
        extra_log_decay.T,
        step_size_bias[None, :],
        log_decay_rate[None, :],
    )
    for d in range(1, parts):
        blocks[d] = lax.ppermute(blocks[d], PLANE, [(i, i ^ d) for i in range(parts)])
    before, total = pl.pallas_call(
        plane_kernel,
        in_specs=[smem] + vmem(parts),
        out_specs=vmem(2),
        out_shape=(sds((parts, height, width), F32), sds((height, width), BF16)),
        scratch_shapes=[pltpu.VMEM((parts, height, width), BF16)],
        compiler_params=params(MID),
        cost_estimate=cost(1000000, MIB),
        name="plane",
    )(place, *blocks)
    zs = lax.axis_size("ep_0")
    planes = lax.all_to_all(
        jnp.broadcast_to(total[None], (zs, height, width)), "ep_0", 0, 0, tiled=True
    )
    entering = pl.pallas_call(
        enter_kernel,
        in_specs=[smem] + vmem(2),
        out_specs=vmem(1)[0],
        out_shape=sds((parts, height - 16, width), BF16),
        compiler_params=params(MID),
        cost_estimate=cost(1000000, MIB),
        name="enter",
    )(lax.axis_index("ep_0").reshape(1).astype(jnp.int32), before, planes)
    entering = lax.all_to_all(entering, PLANE, 0, 0, tiled=True)

    y = pl.pallas_call(
        within_kernel,
        grid=(groups,),
        in_specs=[
            pl.BlockSpec((length, width), lambda g: (0, g)),
            pl.BlockSpec((length, STATE), lambda g: (0, g)),
            pl.BlockSpec((length, STATE), lambda g: (0, g)),
            pl.BlockSpec((heads, length), lambda g: (0, 0)),
            pl.BlockSpec((heads, length), lambda g: (0, 0)),
            pl.BlockSpec((1, heads), lambda g: (0, 0)),
        ],
        out_specs=pl.BlockSpec((length, width), lambda g: (0, g)),
        out_shape=sds((length, channels), F32),
        compiler_params=params(BIG),
        cost_estimate=cost(4 * length * length * channels, 4 * MIB),
        name="within",
    )(x, w, r, cum, step, direct_path_weight[None, :])

    out_dim = mixer_output_weight.shape[1]
    part = length // tps
    tile = 512
    row_block = lambda rows: pl.BlockSpec((rows, tile), lambda j: (0, j))
    whole = lambda a: pl.BlockSpec(a.shape, lambda j: (0,) * a.ndim)
    own, up, dn, opa, opb = pl.pallas_call(
        project_kernel,
        grid=(out_dim // tile,),
        in_specs=[smem]
        + [whole(a) for a in (y, r, entering, cum, gate_logits)]
        + [pl.BlockSpec((channels, tile), lambda j: (0, j))],
        out_specs=(row_block(part), row_block(part), row_block(part), row_block(part // 2), row_block(part // 2)),
        out_shape=(
            sds((part, out_dim), BF16),
            sds((part, out_dim), BF16),
            sds((part, out_dim), BF16),
            sds((part // 2, out_dim), BF16),
            sds((part // 2, out_dim), BF16),
        ),
        scratch_shapes=[pltpu.VMEM((length, channels), BF16)] * 2,
        compiler_params=params(MID),
        cost_estimate=cost(2 * length * channels * out_dim, 6 * MIB),
        name="project",
    )(me, y, r, entering, cum, gate_logits, mixer_output_weight)
    opa = lax.ppermute(opa, "tp", plus)
    opb = lax.ppermute(opb, "tp", minus)
    half = part // 2
    up = jnp.concatenate([(up[:half].astype(F32) + opa.astype(F32)).astype(BF16), up[half:]], axis=0)
    dn = jnp.concatenate([dn[:half], (dn[half:].astype(F32) + opb.astype(F32)).astype(BF16)], axis=0)
    up = lax.ppermute(up, "tp", plus)
    dn = lax.ppermute(dn, "tp", minus)
    mixer_out = pl.pallas_call(
        norm_kernel,
        in_specs=vmem(4),
        out_specs=vmem(1)[0],
        out_shape=sds((part, out_dim), BF16),
        compiler_params=params(MID),
        cost_estimate=cost(1000000, 2 * MIB),
        name="norm",
    )(own, up, dn, mixer_norm_scale[None, :])

    gate_up = (expert_gate_matrix[0], expert_up_matrix[0])
    half = slots // 2
    work = 2 * slots * model * ff
    l0, l1, r0, r1, o0, o1 = ring(arrived[:half], arrived[half:], "tp")
    (near,) = expert_call(
        hidden_near_kernel,
        (me,),
        (arrived, l0, l1, r0, r1, *gate_up),
        (sds((slots, 2 * ff), F32),),
        3 * work // 2,
        BIG,
    )
    h0, h1 = expert_call(
        hidden_kernel,
        (me,),
        (near, o0, o1, *gate_up),
        (sds((half, ff), BF16), sds((half, ff), BF16)),
        work // 2,
    )
    l0, l1, r0, r1, o0, o1 = ring(h0, h1, "tp")
    (near,) = expert_call(
        result_near_kernel,
        (),
        (h0, h1, l0, l1, r0, r1, d_own, d_left, d_right),
        (sds((slots, quarter), F32),),
        3 * work // 4,
    )
    (result,) = expert_call(
        result_kernel, (), (near, o0, o1, d_cross), (sds((slots, quarter), BF16),), work // 4
    )
    returned = lax.all_to_all(
        result.reshape(experts, CAP, quarter), EP, split_axis=0, concat_axis=0, tiled=True
    )
    returned = returned.reshape(slots, quarter)
    expert_out = pl.pallas_call(
        combine_kernel,
        in_specs=vmem(3),
        out_specs=vmem(1)[0],
        out_shape=sds((tokens, quarter), BF16),
        compiler_params=params(MID),
        cost_estimate=cost(4 * slots * tokens * quarter, 2 * MIB),
        name="combine",
    )(returned, dest, routing_weights.T)
    return (mixer_out, expert_out)


def solution(mesh):
    split = Mesh(mesh.devices.reshape(8, 4, 2, mesh.shape["tp"]), EP_TP)
    placed = (
        P(EP, "tp"),
        P(EP, "tp"),
        P(EP, "tp"),
        P(EP, "tp"),
        P(EP, "tp"),
        P(EP, "tp"),
        P(None, "tp"),
        P(None, "tp"),
        P(None, "tp"),
        P("tp"),
        P("tp"),
        P("tp"),
        P("tp", None),
        P(),
        P(EP, None),
        P(),
        P(EP, None),
        P(EP, None),
        P(EP, None, "tp"),
        P(EP, None, "tp"),
        P(EP, "tp", None),
    )

    return jax.shard_map(
        per_device,
        mesh=split,
        in_specs=placed,
        out_specs=(P(EP_TP, None), P(EP, "tp")),
        check_vma=False,
    )
```

```python
import jax
import jax.numpy as jnp
from jax import lax
from jax.experimental import pallas as pl
from jax.experimental.pallas import tpu as pltpu
from jax.sharding import Mesh
from jax.sharding import PartitionSpec as P


HEAD_DIM = 64
STATE = 128
CAP = 16
EP = ("ep_0", "ep_1", "ep_2")
PLANE = ("ep_1", "ep_2")
EP_TP = ("ep_0", "ep_1", "ep_2", "tp")
EPS = 1e-06
F32 = jnp.float32
BF16 = jnp.bfloat16
MIB = 1024 * 1024
BIG = 56
MID = 24


def vmem(count):
    return [pl.BlockSpec(memory_space=pltpu.VMEM)] * count


def params(mib):
    return pltpu.CompilerParams(vmem_limit_bytes=mib * MIB)


def cost(flops, nbytes):
    return pl.CostEstimate(flops=flops, bytes_accessed=nbytes, transcendentals=0)


def iota(shape, dim):
    return lax.broadcasted_iota(jnp.int32, shape, dim)


def spread_heads(group, heads, width):
    per = width // HEAD_DIM
    return (iota((heads, width), 0) == group * per + iota((heads, width), 1) // HEAD_DIM).astype(F32)


def dot(a, b, precision=None):
    return jnp.dot(a, b, preferred_element_type=F32, precision=precision)


def dot_tn(a, b):
    return lax.dot_general(a, b, (((0,), (0,)), ((), ())), preferred_element_type=F32)


def dot_nt(a, b):
    return lax.dot_general(a, b, (((1,), (1,)), ((), ())), preferred_element_type=F32)


def silu(x):
    return 0.5 * x * (1.0 + jnp.tanh(0.5 * x))


def split3(x):
    high = x.astype(BF16)
    rest = x - high.astype(F32)
    middle = rest.astype(BF16)
    low = (rest - middle.astype(F32)).astype(BF16)
    return jnp.concatenate([high, middle, low], axis=0)


def to_lanes(terms, mask):
    return dot_tn(terms, jnp.concatenate([mask.astype(BF16)] * 3, axis=0))


def to_column(row):
    n = row.shape[1]
    return jnp.sum(jnp.where(iota((n, n), 0) == iota((n, n), 1), row, 0.0), axis=1, keepdims=True)


def conv_kernel(
    place_ref, ch_ref, wr_ref, rd_ref, edge_ref, ct_ref, wt_ref, rt_ref, sraw_ref, extra_ref, bias_ref, rate_ref,
    x_ref, w_ref, r_ref, cum_ref, step_ref, *rest,
):
    *block_refs, pay_ref = rest
    heads, length = sraw_ref.shape
    tile = 128

    def conv(src, taps, dst, first):
        def body(i, carry):
            lanes = pl.ds(pl.multiple_of(i * tile, tile), tile)
            edges = edge_ref[:, pl.ds(pl.multiple_of(first + i * tile, tile), tile)].astype(F32)
            joined = jnp.concatenate([edges[8:16], src[:, lanes].astype(F32)], axis=0)
            t = taps[:, lanes]
            total = t[0:1] * joined[5 : 5 + length]
            for k in range(1, t.shape[0]):
                total = total + t[k : k + 1] * joined[5 + k : 5 + k + length]
            dst[:, lanes] = silu(total).astype(BF16)
            return carry

        lax.fori_loop(0, src.shape[1] // tile, body, 0)

    nch, nw = ch_ref.shape[1], wr_ref.shape[1]
    conv(ch_ref, ct_ref, x_ref, 0)
    conv(wr_ref, wt_ref, w_ref, nch)
    conv(rd_ref, rt_ref, r_ref, nch + nw)

    raw = sraw_ref[...].astype(F32) + to_column(bias_ref[...])
    step = jnp.maximum(raw, 0.0) + jnp.log1p(jnp.exp(-jnp.abs(raw)))
    decay = extra_ref[...] - step * to_column(jnp.exp(rate_ref[...]))
    upto = jnp.where(iota((length, length), 0) <= iota((length, length), 1), 1.0, 0.0).astype(BF16)
    sums = dot(split3(decay), upto)
    cum = sums[0:heads] + sums[heads : 2 * heads] + sums[2 * heads :]
    cum_ref[...] = cum
    step_ref[...] = step
    last = cum[:, length - 1 : length]
    tail = split3(jnp.exp(last - cum) * step)
    last = split3(jnp.broadcast_to(last, (heads, 128)))
    groups = nw // STATE
    width = nch // groups
    parts = pay_ref.shape[0]
    rows = STATE // parts
    his, los = [], []
    for g in range(groups):
        spread = spread_heads(g, heads, width)
        xt = (x_ref[:, g * width : (g + 1) * width].astype(F32) * to_lanes(tail, spread)).astype(BF16)
        state = dot_tn(w_ref[:, g * STATE : (g + 1) * STATE], xt).astype(BF16)
        pay_ref[:, g * rows : (g + 1) * rows, :] = state.reshape(parts, rows, width)
        total = to_lanes(last, spread)[0:1]
        high = total.astype(BF16).astype(F32)
        his.append(high)
        los.append(total - high)
    extra_rows = jnp.concatenate(his + los + [jnp.zeros((16 - 2 * groups, width), F32)], axis=0).astype(BF16)
    for p in range(parts):
        pay_ref[p, groups * rows :, :] = extra_rows
    for d in range(parts):
        block_refs[d][...] = pay_ref[jnp.bitwise_xor(place_ref[0], d)]


def within_kernel(x_ref, w_ref, r_ref, cum_ref, step_ref, direct_ref, y_ref):
    g = pl.program_id(0)
    heads, length = cum_ref.shape
    width = x_ref.shape[1]
    per = width // HEAD_DIM
    block = 128
    pick = iota((heads, 128), 0) == g * per + iota((heads, 128), 1)
    cols = to_lanes(split3(cum_ref[...]), pick.astype(F32))
    spread = spread_heads(g, heads, width)
    x = x_ref[...].astype(F32)
    xs = (x * to_lanes(split3(step_ref[...]), spread)).astype(BF16)
    direct = to_lanes(split3(jnp.broadcast_to(to_column(direct_ref[...]), (heads, 128))), spread)[0:1]
    first_half = iota((block, 128), 1) < HEAD_DIM
    causal = iota((block, block), 0) >= iota((block, block), 1)
    rows = [cum_ref[pl.ds(g * per + j, 1), :] for j in range(per)]
    for i in range(length // block):
        here = slice(i * block, (i + 1) * block)
        seen = (i + 1) * block
        gram = dot_nt(r_ref[here, :], w_ref[0:seen, :])
        outs = []
        for j in range(per):
            gap = cols[here, j : j + 1] - rows[j][:, 0:seen]
            edge = jnp.where(causal, gap[:, i * block :], -1e30)
            if i:
                gap = jnp.concatenate([gap[:, : i * block], edge], axis=1)
            else:
                gap = edge
            m = (gram * jnp.exp(gap)).astype(BF16)
            pair = (j // 2) * 128
            outs.append(dot(m, xs[0:seen, pair : pair + 128]))
        for q in range(per // 2):
            lanes = slice(q * 128, (q + 1) * 128)
            y_ref[here, lanes] = (
                jnp.where(first_half, outs[2 * q], outs[2 * q + 1]) + direct[:, lanes] * x[here, lanes]
            )


def plane_kernel(place_ref, *refs):
    *block_refs, before_ref, total_ref, z_ref = refs
    parts, height, width = z_ref.shape
    for d in range(parts):
        z_ref[jnp.bitwise_xor(place_ref[0], d)] = block_refs[d][...]
    groups = 4
    rows = (height - 16) // groups
    base = groups * rows
    his, los = [], []
    for g in range(groups):
        run = jnp.zeros((rows, width), F32)
        log = jnp.zeros((1, width), F32)
        here = slice(g * rows, (g + 1) * rows)
        for p in range(parts):
            before_ref[p, here, :] = run
            before_ref[p, base + g : base + g + 1, :] = log
            pad = z_ref[p, base : base + 16, :].astype(F32)
            own = pad[g : g + 1] + pad[groups + g : groups + g + 1]
            run = jnp.exp(own) * run + z_ref[p, here, :].astype(F32)
            log = log + own
        total_ref[here, :] = run.astype(BF16)
        high = log.astype(BF16).astype(F32)
        his.append(high)
        los.append(log - high)
    total_ref[base:, :] = jnp.concatenate(
        his + los + [jnp.zeros((16 - 2 * groups, width), F32)], axis=0
    ).astype(BF16)


def unpack_logs(ref, groups, base):
    pad = ref[base : base + 16, :].astype(F32)
    return pad[0:groups] + pad[groups : 2 * groups]


def enter_kernel(zi_ref, before_ref, planes_ref, out_ref):
    count, height, width = planes_ref.shape
    parts = before_ref.shape[0]
    groups = 4
    rows = (height - 16) // groups
    base = groups * rows
    mine = zi_ref[0]
    logs = [unpack_logs(planes_ref.at[k], groups, base) for k in range(count)]
    for g in range(groups):
        here = slice(g * rows, (g + 1) * rows)
        state = jnp.zeros((rows, width), F32)
        for k in range(count - 1):
            new = jnp.exp(logs[k][g : g + 1]) * state + planes_ref[k, here, :].astype(F32)
            state = jnp.where(k < mine, new, state)
        for p in range(parts):
            log = before_ref[p, base + g : base + g + 1, :]
            out_ref[p, here, :] = (before_ref[p, here, :] + jnp.exp(log) * state).astype(BF16)


def project_kernel(
    me_ref, y_ref, r_ref, s_ref, cum_ref, gate_ref, wo_ref,
    own_ref, up_ref, down_ref, opa_ref, opb_ref, natural_ref, gated_ref,
):
    heads, length = cum_ref.shape
    n = 4
    part = length // n
    groups = r_ref.shape[1] // STATE
    width = y_ref.shape[1] // groups

    @pl.when(pl.program_id(0) == 0)
    def _():
        me = me_ref[0]
        grown = split3(jnp.exp(cum_ref[...]))
        for g in range(groups):
            lanes = slice(g * width, (g + 1) * width)
            state = s_ref[:, g * 16 : (g + 1) * 16, :].reshape(STATE, width)
            carried = dot(r_ref[:, g * STATE : (g + 1) * STATE], state)
            y = y_ref[:, lanes] + to_lanes(grown, spread_heads(g, heads, width)) * carried
            natural_ref[:, lanes] = (y * silu(gate_ref[:, lanes].astype(F32))).astype(BF16)
        for k in range(n):
            rows = pl.ds(pl.multiple_of(lax.rem(me + k, n) * part, part), part)
            gated_ref[k * part : (k + 1) * part, :] = natural_ref[rows, :]

    out = dot(gated_ref[...], wo_ref[...]).astype(BF16)
    own_ref[...] = out[0:part]
    up_ref[...] = out[part : 2 * part]
    opa_ref[...] = out[2 * part : 2 * part + part // 2]
    opb_ref[...] = out[2 * part + part // 2 : 3 * part]
    down_ref[...] = out[3 * part : 4 * part]


def norm_kernel(own_ref, u_ref, d_ref, gain_ref, out_ref):
    total = own_ref[...].astype(F32) + u_ref[...].astype(F32) + d_ref[...].astype(F32)
    mean = jnp.mean(total * total, axis=-1, keepdims=True)
    out_ref[...] = (total * lax.rsqrt(mean + EPS) * gain_ref[...]).astype(BF16)


def dispatch_kernel(
    me_ref, tok_ref, gain_ref, routes_ref, ch_ref, wr_ref, rd_ref, out_ref, dest_ref, edge_ref
):
    count = tok_ref.shape[0]
    slots, quarter = out_ref.shape
    experts = slots // CAP
    nch, nw = ch_ref.shape[1], wr_ref.shape[1]
    edge_ref[:, 0:nch] = ch_ref[...]
    edge_ref[:, nch : nch + nw] = wr_ref[...]
    edge_ref[:, nch + nw :] = rd_ref[...]
    v = tok_ref[...].astype(F32)
    mean = jnp.mean(v * v, axis=-1, keepdims=True)
    lanes = pl.ds(pl.multiple_of(me_ref[0] * quarter, quarter), quarter)
    normed = (tok_ref[:, lanes].astype(F32) * lax.rsqrt(mean + EPS) * gain_ref[:, lanes]).astype(BF16)
    ids = iota((experts, count), 0)
    is_first, is_second = ids == routes_ref[0:1, :], ids == routes_ref[1:2, :]
    named = jnp.where(is_first | is_second, 1.0, 0.0).astype(BF16)
    before = jnp.where(iota((count, count), 0) < iota((count, count), 1), 1.0, 0.0).astype(BF16)
    place = dot(named, before) + (ids * CAP).astype(F32)
    dest0 = jnp.sum(jnp.where(is_first, place, 0.0), axis=0, keepdims=True).astype(jnp.int32)
    dest1 = jnp.sum(jnp.where(is_second, place, 0.0), axis=0, keepdims=True).astype(jnp.int32)
    dest_ref[0:1, :] = dest0
    dest_ref[1:2, :] = dest1
    slot = iota((slots, count), 0)
    chosen = jnp.where((slot == dest0) | (slot == dest1), 1.0, 0.0).astype(BF16)
    out_ref[...] = dot(chosen, normed).astype(BF16)


def combine_kernel(back_ref, dest_ref, weight_ref, out_ref):
    count = dest_ref.shape[1]
    slot = iota((back_ref.shape[0], count), 0)
    mix = jnp.where(slot == dest_ref[0:1, :], weight_ref[0:1, :], 0.0) + jnp.where(
        slot == dest_ref[1:2, :], weight_ref[1:2, :], 0.0
    )
    high = mix.astype(BF16)
    low = (mix - high.astype(F32)).astype(BF16)
    back = back_ref[...]
    out_ref[...] = (dot_tn(high, back) + dot_tn(low, back)).astype(BF16)


def tp_rows(me, shift, size):
    return pl.ds(pl.multiple_of(lax.rem(me + shift, 4) * size, size), size)


def hidden_near_kernel(me_ref, own, left0, left1, right0, right1, gate_ref, up_ref, out_ref):
    half, size = left0.shape
    columns = gate_ref.shape[1]
    for c, (left, right) in enumerate(((left0, right0), (left1, right1))):
        here = slice(c * half, (c + 1) * half)
        for k, w in enumerate((gate_ref, up_ref)):
            total = dot(own[here, :], w[tp_rows(me_ref[0], 0, size), :])
            total = total + dot(left[...], w[tp_rows(me_ref[0], 3, size), :])
            total = total + dot(right[...], w[tp_rows(me_ref[0], 1, size), :])
            out_ref[here, k * columns : (k + 1) * columns] = total


def hidden_kernel(me_ref, near_ref, op0, op1, gate_ref, up_ref, out0_ref, out1_ref):
    half, size = op0.shape
    columns = gate_ref.shape[1]
    for c, (op, out_ref) in enumerate(((op0, out0_ref), (op1, out1_ref))):
        here = slice(c * half, (c + 1) * half)
        rows = tp_rows(me_ref[0], 2, size)
        gate = near_ref[here, :columns] + dot(op[...], gate_ref[rows, :])
        up = near_ref[here, columns:] + dot(op[...], up_ref[rows, :])
        out_ref[...] = (silu(gate) * up).astype(BF16)


def result_near_kernel(own0, own1, left0, left1, right0, right1, down_own, down_left, down_right, out_ref):
    half = own0.shape[0]
    for c, (own, left, right) in enumerate(((own0, left0, right0), (own1, left1, right1))):
        total = dot(own[...], down_own[...]) + dot(left[...], down_left[...])
        out_ref[c * half : (c + 1) * half, :] = total + dot(right[...], down_right[...])


def result_kernel(near_ref, op, down_ref, *rest):
    rest[-1][...] = (near_ref[...] + dot(op[...], down_ref[...])).astype(BF16)


def result_call(half, near, op, down, before):
    rows, columns = op.shape[0], down.shape[1]
    extra = () if before is None else (before,)
    return pl.pallas_call(
        result_kernel,
        grid=(1,),
        in_specs=[
            pl.BlockSpec((rows, columns), lambda i: (half, 0)),
            pl.BlockSpec(op.shape, lambda i: (0, 0)),
            pl.BlockSpec(down.shape, lambda i: (0, 0)),
        ]
        + [pl.BlockSpec(memory_space=pl.ANY)] * len(extra),
        out_specs=pl.BlockSpec((rows, columns), lambda i: (half, 0)),
        out_shape=jax.ShapeDtypeStruct((2 * rows, columns), BF16),
        input_output_aliases={3: 0} if extra else {},
        compiler_params=params(MID),
        cost_estimate=cost(2 * rows * op.shape[1] * columns, 2 * MIB),
    )(near, op, down, *extra)


def ring_step(x, axis, by):
    n = lax.axis_size(axis)
    return lax.ppermute(x, axis, [(i, (i + by) % n) for i in range(n)])


def ring(first, second, axis):
    left0 = ring_step(first, axis, 1)
    right1 = ring_step(second, axis, -1)
    left1 = ring_step(second, axis, 1)
    right0 = ring_step(first, axis, -1)
    op0 = ring_step(left0, axis, 1)
    op1 = ring_step(right1, axis, -1)
    return left0, left1, right0, right1, op0, op1


def expert_call(kernel, scalars, arrays, shapes, flops, grant=MID):
    return pl.pallas_call(
        kernel,
        in_specs=[pl.BlockSpec(memory_space=pltpu.SMEM)] * len(scalars) + vmem(len(arrays)),
        out_specs=vmem(len(shapes)),
        out_shape=shapes,
        compiler_params=params(grant),
        cost_estimate=cost(flops, 4 * MIB),
    )(*scalars, *arrays)


def per_device(
    mixer_channels_raw,
    write_vectors_raw,
    read_vectors_raw,
    gate_logits,
    step_size_raw,
    extra_log_decay,
    mixer_conv_taps,
    write_conv_taps,
    read_conv_taps,
    step_size_bias,
    log_decay_rate,
    direct_path_weight,
    mixer_output_weight,
    mixer_norm_scale,
    routed_tokens,
    expert_norm_scale,
    routes,
    routing_weights,
    expert_gate_matrix,
    expert_up_matrix,
    expert_down_matrix,
):
    sds = jax.ShapeDtypeStruct
    smem = pl.BlockSpec(memory_space=pltpu.SMEM)
    tp = lax.axis_index("tp")
    me = tp.reshape(1).astype(jnp.int32)
    tps = lax.axis_size("tp")
    plus = [(i, (i + 1) % tps) for i in range(tps)]
    minus = [(i, (i - 1) % tps) for i in range(tps)]
    cross = [(i, (i + 2) % tps) for i in range(tps)]

    tokens, model = routed_tokens.shape
    experts = lax.axis_size(EP)
    slots = experts * CAP
    quarter = model // tps
    length, channels = mixer_channels_raw.shape
    nw = write_vectors_raw.shape[1]
    last_rows = lambda a: pl.BlockSpec((16, a.shape[1]), lambda i: (a.shape[0] // 16 - 1, 0))
    entire = lambda shape: pl.BlockSpec(shape, lambda i: (0,) * len(shape))
    outgoing, dest, edge = pl.pallas_call(
        dispatch_kernel,
        grid=(1,),
        in_specs=[smem, entire((tokens, model)), entire((1, model)), entire((2, tokens))]
        + [last_rows(a) for a in (mixer_channels_raw, write_vectors_raw, read_vectors_raw)],
        out_specs=[entire((slots, quarter)), entire((2, tokens)), entire((16, channels + 2 * nw))],
        out_shape=(
            sds((slots, quarter), BF16),
            sds((2, tokens), jnp.int32),
            sds((16, channels + 2 * nw), BF16),
        ),
        compiler_params=params(BIG),
        cost_estimate=cost(2 * slots * tokens * quarter, 4 * MIB),
        name="dispatch",
    )(
        me,
        routed_tokens,
        expert_norm_scale[None, :],
        routes.T,
        mixer_channels_raw,
        write_vectors_raw,
        read_vectors_raw,
    )
    arrived = lax.all_to_all(
        outgoing.reshape(experts, CAP, quarter), EP, split_axis=0, concat_axis=0, tiled=True
    )
    arrived = arrived.reshape(slots, quarter)

    ff = expert_down_matrix.shape[1]
    down = expert_down_matrix[0]

    def feature_block(shift):
        return lax.dynamic_slice(down, (0, lax.rem(tp + shift, tps) * quarter), (ff, quarter))

    d_own = feature_block(0)
    d_left = lax.ppermute(feature_block(1), "tp", plus)
    d_right = lax.ppermute(feature_block(3), "tp", minus)
    d_cross = lax.ppermute(feature_block(2), "tp", cross)

    heads = step_size_raw.shape[1]
    groups = nw // STATE
    width = channels // groups
    edge = lax.ppermute(edge, EP, [(i, i + 1) for i in range(experts - 1)])
    place = lax.axis_index(PLANE).reshape(1).astype(jnp.int32)
    parts = lax.axis_size(PLANE)
    height = groups * (STATE // parts) + 16
    x, w, r, cum, step, *blocks = pl.pallas_call(
        conv_kernel,
        in_specs=[smem] + vmem(11),
        out_specs=vmem(5 + parts),
        out_shape=(
            sds((length, channels), BF16),
            sds((length, nw), BF16),
            sds((length, nw), BF16),
            sds((heads, length), F32),
            sds((heads, length), F32),
        )
        + (sds((height, width), BF16),) * parts,
        scratch_shapes=[pltpu.VMEM((parts, height, width), BF16)],
        compiler_params=params(BIG),
        cost_estimate=cost(2 * length * STATE * channels * 8, 4 * MIB),
        name="conv",
    )(
        place,
        mixer_channels_raw,
        write_vectors_raw,
        read_vectors_raw,
        edge,
        mixer_conv_taps,
        write_conv_taps,
        read_conv_taps,
        step_size_raw.T,
        extra_log_decay.T,
        step_size_bias[None, :],
        log_decay_rate[None, :],
    )
    for d in range(1, parts):
        blocks[d] = lax.ppermute(blocks[d], PLANE, [(i, i ^ d) for i in range(parts)])
    before, total = pl.pallas_call(
        plane_kernel,
        in_specs=[smem] + vmem(parts),
        out_specs=vmem(2),
        out_shape=(sds((parts, height, width), F32), sds((height, width), BF16)),
        scratch_shapes=[pltpu.VMEM((parts, height, width), BF16)],
        compiler_params=params(MID),
        cost_estimate=cost(1000000, MIB),
        name="plane",
    )(place, *blocks)
    zs = lax.axis_size("ep_0")
    planes = lax.all_to_all(
        jnp.broadcast_to(total[None], (zs, height, width)), "ep_0", 0, 0, tiled=True
    )
    entering = pl.pallas_call(
        enter_kernel,
        in_specs=[smem] + vmem(2),
        out_specs=vmem(1)[0],
        out_shape=sds((parts, height - 16, width), BF16),
        compiler_params=params(MID),
        cost_estimate=cost(1000000, MIB),
        name="enter",
    )(lax.axis_index("ep_0").reshape(1).astype(jnp.int32), before, planes)
    entering = lax.all_to_all(entering, PLANE, 0, 0, tiled=True)

    y = pl.pallas_call(
        within_kernel,
        grid=(groups,),
        in_specs=[
            pl.BlockSpec((length, width), lambda g: (0, g)),
            pl.BlockSpec((length, STATE), lambda g: (0, g)),
            pl.BlockSpec((length, STATE), lambda g: (0, g)),
            pl.BlockSpec((heads, length), lambda g: (0, 0)),
            pl.BlockSpec((heads, length), lambda g: (0, 0)),
            pl.BlockSpec((1, heads), lambda g: (0, 0)),
        ],
        out_specs=pl.BlockSpec((length, width), lambda g: (0, g)),
        out_shape=sds((length, channels), F32),
        compiler_params=params(BIG),
        cost_estimate=cost(4 * length * length * channels, 4 * MIB),
        name="within",
    )(x, w, r, cum, step, direct_path_weight[None, :])

    out_dim = mixer_output_weight.shape[1]
    part = length // tps
    tile = 512
    row_block = lambda rows: pl.BlockSpec((rows, tile), lambda j: (0, j))
    whole = lambda a: pl.BlockSpec(a.shape, lambda j: (0,) * a.ndim)
    own, up, dn, opa, opb = pl.pallas_call(
        project_kernel,
        grid=(out_dim // tile,),
        in_specs=[smem]
        + [whole(a) for a in (y, r, entering, cum, gate_logits)]
        + [pl.BlockSpec((channels, tile), lambda j: (0, j))],
        out_specs=(row_block(part), row_block(part), row_block(part), row_block(part // 2), row_block(part // 2)),
        out_shape=(
            sds((part, out_dim), BF16),
            sds((part, out_dim), BF16),
            sds((part, out_dim), BF16),
            sds((part // 2, out_dim), BF16),
            sds((part // 2, out_dim), BF16),
        ),
        scratch_shapes=[pltpu.VMEM((length, channels), BF16)] * 2,
        compiler_params=params(MID),
        cost_estimate=cost(2 * length * channels * out_dim, 6 * MIB),
        name="project",
    )(me, y, r, entering, cum, gate_logits, mixer_output_weight)
    opa = lax.ppermute(opa, "tp", plus)
    opb = lax.ppermute(opb, "tp", minus)
    half = part // 2
    up = jnp.concatenate([(up[:half].astype(F32) + opa.astype(F32)).astype(BF16), up[half:]], axis=0)
    dn = jnp.concatenate([dn[:half], (dn[half:].astype(F32) + opb.astype(F32)).astype(BF16)], axis=0)
    up = lax.ppermute(up, "tp", plus)
    dn = lax.ppermute(dn, "tp", minus)
    mixer_out = pl.pallas_call(
        norm_kernel,
        in_specs=vmem(4),
        out_specs=vmem(1)[0],
        out_shape=sds((part, out_dim), BF16),
        compiler_params=params(MID),
        cost_estimate=cost(1000000, 2 * MIB),
        name="norm",
    )(own, up, dn, mixer_norm_scale[None, :])

    gate_up = (expert_gate_matrix[0], expert_up_matrix[0])
    half = slots // 2
    work = 2 * slots * model * ff
    l0, l1, r0, r1, o0, o1 = ring(arrived[:half], arrived[half:], "tp")
    (near,) = expert_call(
        hidden_near_kernel,
        (me,),
        (arrived, l0, l1, r0, r1, *gate_up),
        (sds((slots, 2 * ff), F32),),
        3 * work // 2,
        BIG,
    )
    h0, h1 = expert_call(
        hidden_kernel,
        (me,),
        (near, o0, o1, *gate_up),
        (sds((half, ff), BF16), sds((half, ff), BF16)),
        work // 2,
    )
    l0, l1, r0, r1, o0, o1 = ring(h0, h1, "tp")
    (near,) = expert_call(
        result_near_kernel,
        (),
        (h0, h1, l0, l1, r0, r1, d_own, d_left, d_right),
        (sds((slots, quarter), F32),),
        3 * work // 4,
    )
    result = result_call(1, near, o1, d_cross, None)
    result = result_call(0, near, o0, d_cross, result)
    returned = lax.all_to_all(
        result.reshape(experts, CAP, quarter), EP, split_axis=0, concat_axis=0, tiled=True
    )
    returned = returned.reshape(slots, quarter)
    expert_out = pl.pallas_call(
        combine_kernel,
        in_specs=vmem(3),
        out_specs=vmem(1)[0],
        out_shape=sds((tokens, quarter), BF16),
        compiler_params=params(MID),
        cost_estimate=cost(4 * slots * tokens * quarter, 2 * MIB),
        name="combine",
    )(returned, dest, routing_weights.T)
    return (mixer_out, expert_out)


def solution(mesh):
    split = Mesh(mesh.devices.reshape(8, 4, 2, mesh.shape["tp"]), EP_TP)
    placed = (
        P(EP, "tp"),
        P(EP, "tp"),
        P(EP, "tp"),
        P(EP, "tp"),
        P(EP, "tp"),
        P(EP, "tp"),
        P(None, "tp"),
        P(None, "tp"),
        P(None, "tp"),
        P("tp"),
        P("tp"),
        P("tp"),
        P("tp", None),
        P(),
        P(EP, None),
        P(),
        P(EP, None),
        P(EP, None),
        P(EP, None, "tp"),
        P(EP, None, "tp"),
        P(EP, "tp", None),
    )

    return jax.shard_map(
        per_device,
        mesh=split,
        in_specs=placed,
        out_specs=(P(EP_TP, None), P(EP, "tp")),
        check_vma=False,
    )
```
